512 devices in a mesh: grp: 2 (over y), sp: 64 (over z, core), tp: 4 (over x).
Axes of the slice: x: 4, y: 2, z: 32, core: 2. Of those that a mesh axis runs over, the one named last changes fastest.
The devices are a block of a 4x8x32 slice.
Arguments:
- tokens: bfloat16 [131072, 2048], P(('grp', 'sp', 'tp')), parts along dimension 0, may hold values from -6 to 6
- step: float32 [131072], P(('grp', 'sp')), parts along dimension 0, may hold values from 0.2 to 3.75
- in_gain: float32 [2048], replicated, may hold values from 0.1 to 1.9
- in_proj: bfloat16 [2048, 512], P(None, 'tp'), may hold values from -0.125 to 0.125
- decay_rate: float32 [32, 64], P('tp'), may hold values from 1.5258789e-06 to 0.04
- frequency: float32 [32, 64], P('tp'), may hold values from 0.2 to 3
- input_map: float32 [2, 32, 64, 16], P(None, 'tp'), may hold values from -1 to 1
- readout: float32 [2, 32, 16, 64], P(None, 'tp'), may hold values from -0.75 to 0.75
- out_gain: float32 [512], replicated, may hold values from 0.1 to 1.9
- out_proj: bfloat16 [512, 2048], replicated, may hold values from -0.25 to 0.25
Outputs:
- mixed: bfloat16 [131072, 2048], P(('grp', 'sp', 'tp')), parts along dimension 0
The draws below stay inside these ranges and needn't reach their ends.
There are 2 independent parts, one for each index of `grp`. The reference program is written for one: setup_inputs(seed, part) draws one part's arguments, and reference() takes and returns one part's arrays. A program takes and returns all parts, laid end to end along the dimension named above; an argument that names none is the same for every part. Nothing has to cross between parts.
All inputs are finite; a program needn't handle non-finite values.
Results may differ from the reference program's by a relative error of at most 0.01.
Values may be sent and summed in bfloat16 or wider, within the bound.
No kernel may reach another device: no remote copies, remote signals or barrier semaphores. Data moves between devices by JAX's collectives and lax.ppermute only.
A program may use at most 64 MiB of HBM per device.

```python
import jax
import jax.numpy as jnp
from jax import lax

D = 2048
CHANNELS = 512
GROUP_CH = 16
STATE = 64
GROUPS = 32
SEQ_DEV = 1024
TOKENS = 65536


def draw_step(key, part):
    level_key, fine_key = jax.random.split(key)
    levels = jnp.exp(jax.random.uniform(level_key, (TOKENS // SEQ_DEV,), jnp.float32, jnp.log(0.4), jnp.log(2.5)))
    fine = jnp.clip(1.0 + 0.25 * jax.random.normal(fine_key, (TOKENS,), jnp.float32), 0.5, 1.5)
    return jnp.repeat(levels, SEQ_DEV, total_repeat_length=TOKENS) * fine


def draw_decay_rate(key, part):
    pick_key, slow_key, fast_key = jax.random.split(key, 3)
    share = 0.5
    slow_mask = jax.random.uniform(pick_key, (GROUPS, STATE), jnp.float32) < share
    slow = jnp.exp(jax.random.uniform(slow_key, (GROUPS, STATE), jnp.float32, jnp.log(0.1), 0.0)) / TOKENS
    fast = jnp.exp(jax.random.uniform(fast_key, (GROUPS, STATE), jnp.float32, jnp.log(0.01), jnp.log(0.04)))
    return jnp.where(slow_mask, slow, fast)


def block_scale(rng, shape, pieces, low, top_value):
    factor_of, own = 1.0, jax.random.fold_in(rng, 6)
    for dim, blocks in pieces:
        heights = jnp.exp(jax.random.uniform(jax.random.fold_in(own, dim), (blocks,), jnp.float32, low / len(pieces), top_value / len(pieces)))
        factor_of = factor_of * jnp.repeat(heights, shape[dim] // blocks).reshape([-1 if axis == dim else 1 for axis in range(len(shape))])
    return factor_of


def gaussian(rng, shape, deviation, limit, cuts=(), kind=jnp.bfloat16):
    drawn = jax.random.normal(rng, shape, jnp.float32) * deviation
    if len(cuts) > 0:
        drawn = block_scale(rng, shape, cuts, -0.22, 0.18) * drawn
    return jnp.clip(drawn, min=-limit, max=limit).astype(kind)


def setup_inputs(seed: int = 0, part: int = 0) -> dict:
    splits = jax.random.split(jax.random.key(seed), 11)
    part_splits = jax.random.split(jax.random.fold_in(splits[10], part), 11)
    return {
        "tokens": gaussian(part_splits[0], (TOKENS, D), 1.0, 6.0, ((0, 256),)),
        "step": draw_step(jax.random.fold_in(jax.random.fold_in(splits[10], part), 71), part),
        "in_gain": jnp.clip(1.0 + 0.18 * jax.random.normal(splits[2], (D,), jnp.float32), 0.1, 1.9),
        "in_proj": gaussian(splits[3], (D, CHANNELS), D ** -0.5, 0.125, ((1, 4),)),
        "decay_rate": draw_decay_rate(jax.random.fold_in(splits[10], 71), part),
        "frequency": jnp.clip(0.2 + 2.8 * jax.random.uniform(splits[5], (GROUPS, STATE), jnp.float32) ** block_scale(splits[5], (GROUPS, STATE), ((0, 4),), -0.2, 0.2), 0.2, 3.0),
        "input_map": gaussian(splits[6], (2, GROUPS, STATE, GROUP_CH), (2 * GROUP_CH) ** -0.5, 1.0, ((1, 4),), jnp.float32),
        "readout": gaussian(splits[7], (2, GROUPS, GROUP_CH, STATE), STATE ** -0.5, 0.75, ((1, 4),), jnp.float32),
        "out_gain": jnp.clip(1.0 + 0.18 * jax.random.normal(splits[8], (CHANNELS,), jnp.float32), 0.1, 1.9),
        "out_proj": gaussian(splits[9], (CHANNELS, D), CHANNELS ** -0.5, 0.25),
    }


HIGHEST = lax.Precision.HIGHEST

def compose(earlier, later):
    a_re, a_im, b_re, b_im = earlier
    c_re, c_im, d_re, d_im = later
    return (c_re * a_re - c_im * a_im, c_re * a_im + c_im * a_re, c_re * b_re - c_im * b_im + d_re, c_re * b_im + c_im * b_re + d_im)

def rms_rows(values, gain):
    values = values.astype(jnp.float32)
    scaled = values * lax.rsqrt(lax.optimization_barrier(jnp.mean(values * values, axis=-1, keepdims=True)) + 1e-06)
    return (scaled * gain).astype(jnp.bfloat16)

def transition(times, decay_rate, frequency):
    spans = times.astype(jnp.float32)[:, None, None]
    magnitude = jnp.exp(-decay_rate[None] * spans)
    a_re = magnitude * jnp.cos(frequency[None] * spans)
    a_im = magnitude * jnp.sin(frequency[None] * spans)
    lam_re = -decay_rate
    denom = lam_re * lam_re + frequency * frequency
    n_re = a_re - 1.0
    z_re = (n_re * lam_re + a_im * frequency) / denom
    z_im = (a_im * lam_re - n_re * frequency) / denom
    return (a_re, a_im, z_re, z_im)

def injection(drive, input_map, z_re, z_im):
    groups = input_map.shape[1]
    grouped = drive.astype(jnp.float32).reshape(drive.shape[0], groups, -1)
    push_re = jnp.einsum('tgh,gph->tgp', grouped, input_map[0], precision=HIGHEST)
    push_im = jnp.einsum('tgh,gph->tgp', grouped, input_map[1], precision=HIGHEST)
    return (z_re * push_re - z_im * push_im, z_re * push_im + z_im * push_re)

def response(s_re, s_im, readout):
    value = jnp.einsum('tgp,ghp->tgh', s_re, readout[0], precision=HIGHEST) - jnp.einsum('tgp,ghp->tgh', s_im, readout[1], precision=HIGHEST)
    value = value.reshape(s_re.shape[0], -1)
    return jax.nn.gelu(value, approximate=True).astype(jnp.bfloat16)

def reference(tokens, step, in_gain, in_proj, decay_rate, frequency, input_map, readout, out_gain, out_proj):
    normed = rms_rows(tokens, in_gain)
    drive = jnp.dot(normed, in_proj, preferred_element_type=jnp.float32).astype(jnp.bfloat16)
    block_count = TOKENS // SEQ_DEV
    drive_blocks = drive.reshape(block_count, SEQ_DEV, -1)
    time_blocks = step.reshape(block_count, SEQ_DEV)
    zero = jnp.zeros(decay_rate.shape, jnp.float32)

    def advance(carry, piece):
        drive_part, time_part = piece
        a_re, a_im, z_re, z_im = transition(time_part, decay_rate, frequency)
        i_re, i_im = injection(drive_part, input_map, z_re, z_im)
        c_re, c_im, s_re, s_im = lax.associative_scan(compose, (a_re, a_im, i_re, i_im), axis=0)
        s_re = s_re + c_re * carry[0] - c_im * carry[1]
        s_im = s_im + c_re * carry[1] + c_im * carry[0]
        return ((s_re[-1], s_im[-1]), response(s_re, s_im, readout))
    _, answer = lax.scan(advance, (zero, zero), (drive_blocks, time_blocks))
    answer = answer.reshape(TOKENS, -1)
    shaped = rms_rows(answer, out_gain)
    return jnp.dot(shaped, out_proj, preferred_element_type=jnp.float32).astype(jnp.bfloat16)
```

```python
from functools import partial

import jax
import jax.numpy as jnp
from jax import lax
from jax.experimental import pallas as pl
from jax.experimental.pallas import tpu as pltpu
from jax.sharding import Mesh, PartitionSpec as P

CHUNK = 128
LANES = 128
F32 = jnp.float32
BF16 = jnp.bfloat16
TWO_PI_HIGH = 6.28125
TWO_PI_LOW = 0.0019353071795864769
INV_TWO_PI = 0.15915494309189535
SIN = (6.2831854820251465, -41.3416862487793, 81.60456085205078, -76.69428253173828,
       41.96574020385742, -14.708574295043945, 3.0096182823181152)
COS = (1.0, -19.739208221435547, 64.9393539428711, -85.45588684082031, 60.23442077636719,
       -26.364990234375, 7.6985273361206055, -1.3503994941711426)
HIGHEST = lax.Precision.HIGHEST


def polynomial(x, factors):
    total = factors[-1] * x + factors[-2]
    for factor in factors[-3::-1]:
        total = total * x + factor
    return total


def split_turns(freq):
    plain = freq * INV_TWO_PI
    high = jnp.round(plain * 8192.0) * (1.0 / 8192.0)
    rest = (freq - high * TWO_PI_HIGH) - high * TWO_PI_LOW
    return high, rest * INV_TWO_PI, plain


def rotation(coarse, fine, turns, again=False):
    high, rest, plain = turns
    whole = coarse * high
    part = (whole - jnp.round(whole)) + (coarse * rest + fine * plain)
    if again:
        part = part - jnp.round(part)
    square = part * part
    return polynomial(square, COS), part * polynomial(square, SIN)


def decayed(coarse, fine, rate, turns):
    cosine, sine = rotation(coarse, fine, turns, again=True)
    magnitude = jnp.exp(-rate * (coarse + fine))
    return magnitude * cosine, magnitude * sine


def high_low(x):
    high = x.astype(BF16)
    return high, (x - high.astype(F32)).astype(BF16)


def dot_t(a, b):
    return lax.dot_general(a, b, (((1,), (1,)), ((), ())), preferred_element_type=F32)


def tables_kernel(coarse_ref, fine_ref, rate_ref, freq_ref, w_re, w_im, c_re, c_im):
    coarse, fine = coarse_ref[...], fine_ref[...]
    elapsed = coarse + fine
    first = lax.broadcasted_iota(jnp.int32, (CHUNK, LANES), 0) == 0
    for b in range(rate_ref.shape[1] // LANES):
        cols = slice(b * LANES, (b + 1) * LANES)
        rate = rate_ref[:, cols]
        cosine, sine = rotation(coarse, fine, split_turns(freq_ref[:, cols]))
        exponent = rate * elapsed
        shrink = jnp.exp(-exponent)
        c_re[:, cols] = shrink * cosine
        c_im[:, cols] = shrink * sine
        grow = jnp.exp(exponent)
        g_re = grow * cosine
        g_im = -(grow * sine)
        w_re[:, cols] = jnp.where(first, 1.0, pltpu.roll(g_re, 1, 0)) - g_re
        w_im[:, cols] = jnp.where(first, 0.0, pltpu.roll(g_im, 1, 0)) - g_im


def tables(coarse, fine, rate, freq):
    rows, width = coarse.shape[0], rate.shape[1]
    column = pl.BlockSpec((CHUNK, 1), lambda c: (c, 0))
    whole = pl.BlockSpec((1, width), lambda c: (0, 0))
    block = pl.BlockSpec((CHUNK, width), lambda c: (c, 0))
    out = jax.ShapeDtypeStruct((rows, width), F32)
    return pl.pallas_call(
        tables_kernel, grid=(rows // CHUNK,), in_specs=[column, column, whole, whole],
        out_specs=[block] * 4, out_shape=[out] * 4, name="tables",
        cost_estimate=pl.CostEstimate(flops=rows * width * 60, transcendentals=0, bytes_accessed=rows * width * 16),
    )(coarse, fine, rate, freq)


def sums_kernel(at_ref, d0, d1, d2, d3, w_re, w_im, c_re, c_im, push_re, push_im, shift_ref,
                rate4, freq4, acc_re, acc_im, own_ref, sent_ref, push, carry):
    chunk = pl.program_id(0)
    blocks = push_re.shape[0] // LANES

    @pl.when(chunk == 0)
    def _():
        carry[...] = jnp.zeros_like(carry)
        for b in range(blocks):
            rows = slice(b * LANES, (b + 1) * LANES)
            re_high, re_low = high_low(push_re[rows, :])
            im_high, im_low = high_low(push_im[rows, :])
            push[b, :LANES, :LANES] = re_high
            push[b, :LANES, LANES:] = re_low
            push[b, LANES:, :LANES] = im_high
            push[b, LANES:, LANES:] = im_low

    per_slot = d0.shape[0] // CHUNK
    slot = (chunk // per_slot - at_ref[0] + 4) % 4
    start = (chunk % per_slot) * CHUNK
    rows = pl.ds(pl.multiple_of(start, CHUNK), CHUNK)
    drive = jnp.where(slot == 0, d0[rows, :], jnp.where(slot == 1, d1[rows, :],
                      jnp.where(slot == 2, d2[rows, :], d3[rows, :])))
    twice = jnp.concatenate([drive, drive], axis=1)
    row = lax.broadcasted_iota(jnp.int32, (CHUNK, 2 * CHUNK), 0)
    col = lax.broadcasted_iota(jnp.int32, (CHUNK, 2 * CHUNK), 1)
    lower = jnp.where((col % CHUNK) <= row, 1.0, 0.0).astype(BF16)
    for b in range(blocks):
        cols = slice(b * LANES, (b + 1) * LANES)
        pushed = dot_t(twice, push[b])
        p_re, p_im = pushed[:, :LANES], pushed[:, LANES:]
        wr, wi = w_re[:, cols], w_im[:, cols]
        xr_high, xr_low = high_low(wr * p_re - wi * p_im)
        xi_high, xi_low = high_low(wr * p_im + wi * p_re)
        stacked = jnp.concatenate([jnp.concatenate([xr_high, xi_high], axis=1),
                                   jnp.concatenate([xr_low, xi_low], axis=1)], axis=0)
        acc = jnp.dot(lower, stacked, preferred_element_type=F32)
        acc_re[:, cols] = acc[:, :LANES]
        acc_im[:, cols] = acc[:, LANES:]
        cr, ci = c_re[7:8, cols], c_im[7:8, cols]
        tr = acc[CHUNK - 1:, :LANES] + carry[b:b + 1, :]
        ti = acc[CHUNK - 1:, LANES:] + carry[blocks + b:blocks + b + 1, :]
        carry[b:b + 1, :] = cr * tr - ci * ti
        carry[blocks + b:blocks + b + 1, :] = cr * ti + ci * tr

    @pl.when(chunk == pl.num_programs(0) - 1)
    def _():
        own = carry[...]
        own_ref[...] = own
        coarse = shift_ref[0:1, 0:1]
        fine = shift_ref[0:1, 1:2]
        dr, di = decayed(coarse, fine, rate4[...], split_turns(freq4[...]))
        sr, si = own[:blocks], own[blocks:]
        times = shift_ref[...][:, :LANES]
        parts = [times[:, 2:3], times[:, 3:4]]
        lane = lax.broadcasted_iota(jnp.int32, (8, LANES), 1)
        packed = jnp.zeros((8, LANES), F32)
        for k in range(2):
            left = parts[k]
            for j in range(3):
                piece = left.astype(BF16).astype(F32)
                packed = jnp.where(lane == 3 * k + j, piece, packed)
                left = left - piece
        message = jnp.concatenate([dr * sr - di * si, dr * si + di * sr, packed], axis=0).astype(BF16)
        for k in range(sent_ref.shape[0]):
            sent_ref[k] = message


def sums(at, drives, table, push_re, push_im, shift, rate4, freq4, peers):
    w_re, w_im, c_re, c_im = table
    rows, width = w_re.shape
    blocks = width // LANES
    block = pl.BlockSpec((CHUNK, width), lambda c, at: (c, 0))
    last = pl.BlockSpec((8, width), lambda c, at: ((c + 1) * (CHUNK // 8) - 1, 0))

    def whole(array):
        return pl.BlockSpec(array.shape, lambda c, at: (0,) * array.ndim)

    big = jax.ShapeDtypeStruct((rows, width), F32)
    own = jax.ShapeDtypeStruct((2 * blocks, LANES), F32)
    sent = jax.ShapeDtypeStruct((peers, 2 * blocks + 8, LANES), BF16)
    return pl.pallas_call(
        sums_kernel,
        grid_spec=pltpu.PrefetchScalarGridSpec(
            num_scalar_prefetch=1, grid=(rows // CHUNK,),
            in_specs=[whole(d) for d in drives] + [block, block, last, last]
            + [whole(x) for x in (push_re, push_im, shift, rate4, freq4)],
            out_specs=[block, block, pl.BlockSpec(own.shape, lambda c, at: (0, 0)),
                       pl.BlockSpec(sent.shape, lambda c, at: (0, 0, 0))],
            scratch_shapes=[pltpu.VMEM((blocks, 2 * LANES, 2 * push_re.shape[1]), BF16),
                            pltpu.VMEM((2 * blocks, LANES), F32)],
        ),
        out_shape=[big, big, own, sent], name="sums",
        cost_estimate=pl.CostEstimate(flops=rows * width * 1500, transcendentals=0, bytes_accessed=rows * width * 16),
    )(at, *drives, w_re, w_im, c_re, c_im, push_re, push_im, shift, rate4, freq4)


def before_kernel(at_ref, heard_ref, rate4, freq4, own_ref, out_ref):
    rate = rate4[...]
    turns = split_turns(freq4[...])
    blocks = rate.shape[0]
    sr = jnp.zeros(rate.shape, F32)
    si = jnp.zeros(rate.shape, F32)
    for k in range(heard_ref.shape[0] - 1):
        heard = heard_ref[k].astype(F32)
        times = heard[2 * blocks:2 * blocks + 1]
        coarse = (times[:, 0:1] + times[:, 1:2]) + times[:, 2:3]
        fine = (times[:, 3:4] + times[:, 4:5]) + times[:, 5:6]
        dr, di = decayed(coarse, fine, rate, turns)
        nr = dr * sr - di * si + heard[:blocks]
        ni = dr * si + di * sr + heard[blocks:2 * blocks]
        earlier = k < at_ref[1]
        sr = jnp.where(earlier, nr, sr)
        si = jnp.where(earlier, ni, si)
    out_ref[:blocks] = sr
    out_ref[blocks:2 * blocks] = si
    out_ref[2 * blocks:] = own_ref[...]


def before(at, heard, rate4, freq4, own):
    def whole(array):
        return pl.BlockSpec(array.shape, lambda c, at: (0,) * array.ndim)

    out = jax.ShapeDtypeStruct((2 * own.shape[0], LANES), F32)
    return pl.pallas_call(
        before_kernel,
        grid_spec=pltpu.PrefetchScalarGridSpec(
            num_scalar_prefetch=1, grid=(1,), in_specs=[whole(x) for x in (heard, rate4, freq4, own)],
            out_specs=pl.BlockSpec(out.shape, lambda c, at: (0, 0)),
        ),
        out_shape=out, name="before",
    )(at, heard, rate4, freq4, own)


def answer_kernel(at_ref, mine_ref, other_ref, acc_re, acc_im, c_re, c_im, read_re, read_im,
                  shift_ref, rate4, freq4, out_ref, read, carry):
    chunk = pl.program_id(0)
    blocks = rate4.shape[0]

    @pl.when(chunk == 0)
    def _():
        for b in range(blocks):
            cols = slice(b * LANES, (b + 1) * LANES)
            re_high, re_low = high_low(read_re[:, cols])
            im_high, im_low = high_low(-read_im[:, cols])
            read[b, :LANES, :LANES] = re_high
            read[b, :LANES, LANES:] = im_high
            read[b, LANES:, :LANES] = re_low
            read[b, LANES:, LANES:] = im_low
        both = mine_ref[:2 * blocks] + other_ref[:2 * blocks]
        sr, si = both[:blocks], both[blocks:]
        dr, di = decayed(shift_ref[0:1, 4:5], shift_ref[0:1, 5:6], rate4[...], split_turns(freq4[...]))
        second = at_ref[2] == 1
        carry[:blocks] = jnp.where(second, dr * sr - di * si + other_ref[2 * blocks:3 * blocks], sr)
        carry[blocks:] = jnp.where(second, dr * si + di * sr + other_ref[3 * blocks:], si)

    total = jnp.zeros((CHUNK, 2 * LANES), F32)
    for b in range(blocks):
        cols = slice(b * LANES, (b + 1) * LANES)
        tr = acc_re[:, cols] + carry[b:b + 1, :]
        ti = acc_im[:, cols] + carry[blocks + b:blocks + b + 1, :]
        cr, ci = c_re[:, cols], c_im[:, cols]
        sr = cr * tr - ci * ti
        si = cr * ti + ci * tr
        carry[b:b + 1, :] = sr[CHUNK - 1:]
        carry[blocks + b:blocks + b + 1, :] = si[CHUNK - 1:]
        r_high, r_low = high_low(sr)
        i_high, i_low = high_low(si)
        high = jnp.concatenate([r_high, i_high], axis=1)
        low = jnp.concatenate([r_low, i_low], axis=1)
        total = total + dot_t(high, read[b])
        total = total + jnp.concatenate(
            [dot_t(low, read[b, :LANES]), jnp.zeros((CHUNK, LANES), F32)], axis=1)
    value = total[:, :LANES] + total[:, LANES:]
    inner = 0.7978845608 * (value + 0.044715 * (value * value * value))
    out_ref[...] = (0.5 * value * (1.0 + jnp.tanh(inner))).astype(BF16)


def answers(at, mine, other, acc_re, acc_im, c_re, c_im, read_re, read_im, shift, rate4, freq4):
    rows, width = acc_re.shape
    blocks = width // LANES
    block = pl.BlockSpec((CHUNK, width), lambda c, at: (c, 0))

    def whole(array):
        return pl.BlockSpec(array.shape, lambda c, at: (0,) * array.ndim)

    return pl.pallas_call(
        answer_kernel,
        grid_spec=pltpu.PrefetchScalarGridSpec(
            num_scalar_prefetch=1, grid=(rows // CHUNK,),
            in_specs=[whole(mine), whole(other)] + [block] * 4
            + [whole(x) for x in (read_re, read_im, shift, rate4, freq4)],
            out_specs=pl.BlockSpec((CHUNK, LANES), lambda c, at: (c, 0)),
            scratch_shapes=[pltpu.VMEM((blocks, 2 * LANES, 2 * LANES), BF16),
                            pltpu.VMEM((2 * blocks, LANES), F32)],
        ),
        out_shape=jax.ShapeDtypeStruct((rows, LANES), BF16), name="answers",
        cost_estimate=pl.CostEstimate(flops=rows * width * 1000, transcendentals=0, bytes_accessed=rows * width * 16),
    )(at, mine, other, acc_re, acc_im, c_re, c_im, read_re, read_im, shift, rate4, freq4)


def rms_rows(values, gain):
    values = values.astype(F32)
    scaled = values * lax.rsqrt(jnp.mean(values * values, axis=-1, keepdims=True) + 1e-06)
    return (scaled * gain).astype(BF16)


def elapsed_parts(step):
    times = step.reshape(-1, CHUNK)
    grid = jnp.round(times * 8192.0) * (1.0 / 8192.0)
    rows = lax.broadcasted_iota(jnp.int32, (CHUNK, CHUNK), 0)
    cols = lax.broadcasted_iota(jnp.int32, (CHUNK, CHUNK), 1)
    upper = (rows <= cols).astype(F32)
    run = jnp.dot(grid, upper, precision=HIGHEST)
    rest = jnp.dot(times - grid, upper, precision=HIGHEST)
    coarse = jnp.round(run * 8.0) * 0.125
    fine = (run - coarse) + rest
    whole = jnp.sum(coarse[:, -1])
    left = jnp.sum(fine[:, -1])
    return coarse.reshape(-1, 1), fine.reshape(-1, 1), whole, left


def settle(whole, left):
    coarse = jnp.round(whole * 0.5) * 2.0
    return coarse, (whole - coarse) + left


def ring(count, by):
    return [(k, (k + by) % count) for k in range(count)]


def on_device(
    tokens, step, in_gain, in_proj, decay_rate, frequency, input_map, readout, out_gain, out_proj
):
    peers = lax.axis_size("z")
    ways = lax.axis_size("tp")
    core = lax.axis_index("core")
    at = jnp.stack([lax.axis_index("tp"), lax.axis_index("z"), core]).astype(jnp.int32)
    weights = {shift: lax.ppermute(in_proj, "tp", ring(ways, shift)) for shift in (2, 1, 3)}

    coarse, fine, whole, left = elapsed_parts(step)
    times = jnp.zeros((8, LANES), F32).at[0, 0].set(whole).at[0, 1].set(left)
    partner = lax.ppermute(times, "core", [(0, 1), (1, 0)])
    near_whole, near_left = partner[0, 0], partner[0, 1]
    near = settle(near_whole, near_left)
    chip = settle(whole + near_whole, left + near_left)
    first = (core == 0).astype(F32)
    shift = jnp.stack([near[0] * first, near[1] * first, *chip, *near])
    shift = jnp.broadcast_to(jnp.pad(shift, (0, LANES - 6))[None], (8, LANES))

    rate = decay_rate.reshape(1, -1)
    freq = frequency.reshape(1, -1)
    rate4 = decay_rate.reshape(-1, LANES)
    freq4 = frequency.reshape(-1, LANES)
    table = tables(coarse, fine, rate, freq)

    groups, entries = decay_rate.shape
    members = input_map.shape[-1]
    unit = jnp.eye(groups, dtype=F32)
    denom = decay_rate * decay_rate + frequency * frequency
    lam_re = (-decay_rate / denom)[..., None]
    lam_im = (-frequency / denom)[..., None]
    push_re = lam_re * input_map[0] - lam_im * input_map[1]
    push_im = lam_re * input_map[1] + lam_im * input_map[0]

    def spread(small):
        return (small[:, :, None, :] * unit[:, None, :, None]).reshape(groups * entries, groups * members)

    def spread_read(small):
        return (small[:, :, None, :] * unit[:, None, :, None]).reshape(groups * members, groups * entries)

    normed = rms_rows(tokens, in_gain)

    def driven(proj):
        return jnp.dot(normed, proj, preferred_element_type=F32).astype(BF16)

    drives = [driven(in_proj)] + [
        lax.ppermute(driven(weights[k]), "tp", ring(ways, -k)) for k in range(1, ways)
    ]
    acc_re, acc_im, own, sent = sums(
        at, drives, table, spread(push_re), spread(push_im), shift, rate4, freq4, peers
    )
    heard = lax.all_to_all(sent, "z", 0, 0, tiled=True)
    mine = before(at, heard, rate4, freq4, own)
    other = lax.ppermute(mine, "core", [(0, 1), (1, 0)])
    answer = answers(
        at, mine, other, acc_re, acc_im, table[2], table[3],
        spread_read(readout[0]), spread_read(readout[1]), shift, rate4, freq4,
    )
    gathered = lax.all_to_all(answer, "tp", split_axis=0, concat_axis=1, tiled=True)
    shaped = rms_rows(gathered, out_gain)
    return jnp.dot(shaped, out_proj, preferred_element_type=F32).astype(BF16)


def solution(mesh):
    shape = mesh.shape
    devices = mesh.devices.reshape(shape["grp"], shape["sp"] // 2, 2, shape["tp"])
    fine_mesh = Mesh(devices, ("grp", "z", "core", "tp"))
    rows = ("grp", "z", "core", "tp")
    placed = (
        P(rows, None),
        P(("grp", "z", "core")),
        P(),
        P(None, "tp"),
        P("tp", None),
        P("tp", None),
        P(None, "tp", None, None),
        P(None, "tp", None, None),
        P(),
        P(),
    )
    return jax.shard_map(
        on_device,
        mesh=fine_mesh,
        in_specs=placed,
        out_specs=P(rows, None),
        check_vma=False,
    )
```

```python
from functools import partial

import jax
import jax.numpy as jnp
from jax import lax
from jax.experimental import pallas as pl
from jax.experimental.pallas import tpu as pltpu
from jax.sharding import Mesh, PartitionSpec as P

CHUNK = 128
LANES = 128
BLOCK = 8
F32 = jnp.float32
BF16 = jnp.bfloat16
TWO_PI_HIGH = 6.28125
TWO_PI_LOW = 0.0019353071795864769
INV_TWO_PI = 0.15915494309189535
SIN = (6.2831854820251465, -41.3416862487793, 81.60456085205078, -76.69428253173828,
       41.96574020385742, -14.708574295043945, 3.0096182823181152)
COS = (1.0, -19.739208221435547, 64.9393539428711, -85.45588684082031, 60.23442077636719,
       -26.364990234375, 7.6985273361206055, -1.3503994941711426)


def polynomial(x, factors):
    total = factors[-1] * x + factors[-2]
    for factor in factors[-3::-1]:
        total = total * x + factor
    return total


def split_turns(freq):
    plain = freq * INV_TWO_PI
    high = jnp.round(plain * 8192.0) * (1.0 / 8192.0)
    rest = (freq - high * TWO_PI_HIGH) - high * TWO_PI_LOW
    return high, rest * INV_TWO_PI, plain


def rotation(coarse, fine, turns, again=False):
    high, rest, plain = turns
    whole = coarse * high
    part = (whole - jnp.round(whole)) + (coarse * rest + fine * plain)
    if again:
        part = part - jnp.round(part)
    square = part * part
    return polynomial(square, COS), part * polynomial(square, SIN)


def decayed(coarse, fine, rate, turns):
    cosine, sine = rotation(coarse, fine, turns, again=True)
    magnitude = jnp.exp(-rate * (coarse + fine))
    return magnitude * cosine, magnitude * sine


def high_low(x):
    high = x.astype(BF16)
    return high, (x - high.astype(F32)).astype(BF16)


def dot_t(a, b):
    return lax.dot_general(a, b, (((1,), (1,)), ((), ())), preferred_element_type=F32)


def whole(array):
    return pl.BlockSpec(array.shape, lambda *at: (0,) * array.ndim)


def iota(shape, dim):
    return lax.broadcasted_iota(jnp.int32, shape, dim)


def triangle(repeat=1):
    shape = (CHUNK, repeat * CHUNK)
    return jnp.where((iota(shape, 1) % CHUNK) <= iota(shape, 0), 1.0, 0.0).astype(BF16)


def tables_kernel(step_ref, rate_ref, freq_ref, map_ref, readout_ref, w_re, w_im, c_re, c_im,
                  push_ref, read_ref, modes_ref, times_ref):
    chunk = pl.program_id(0)
    blocks = modes_ref.shape[0] // 2
    per_block, entries = rate_ref.shape[0] // blocks, rate_ref.shape[1]

    @pl.when(chunk == 0)
    def _():
        times_ref[...] = jnp.zeros_like(times_ref)
        for b in range(blocks):
            mine = range(per_block * b, per_block * (b + 1))
            modes_ref[b:b + 1, :] = jnp.concatenate([rate_ref[g:g + 1, :] for g in mine], axis=1)
            modes_ref[blocks + b:blocks + b + 1, :] = jnp.concatenate([freq_ref[g:g + 1, :] for g in mine], axis=1)

    for b in range(blocks):
        @pl.when(chunk == b)
        def _(b=b):
            read_ref[b] = jnp.zeros(read_ref.shape[1:], BF16)
            for j in range(per_block):
                g = per_block * b + j
                members = map_ref.shape[-1]
                place = (iota((members, LANES), 1) == iota((members, LANES), 0) + members * g)
                place = jnp.where(place, 1.0, 0.0).astype(BF16)
                seat = (iota((entries, LANES), 1) == iota((entries, LANES), 0) + entries * j)
                seat = jnp.where(seat, 1.0, 0.0).astype(BF16)
                for part in range(2):
                    rows = slice(part * LANES + entries * j, part * LANES + entries * (j + 1))
                    for k, piece in enumerate(high_low(map_ref[part, g])):
                        spread = jnp.dot(piece, place, preferred_element_type=F32)
                        push_ref[b, rows, k * LANES:(k + 1) * LANES] = spread.astype(BF16)
                    sign = 1.0 if part == 0 else -1.0
                    for k, piece in enumerate(high_low(sign * readout_ref[part, g])):
                        spread = jnp.dot(piece, seat, preferred_element_type=F32)
                        first = k * LANES + members * g
                        read_ref[b, first:first + members, part * LANES:(part + 1) * LANES] = spread.astype(BF16)

    lower = triangle()
    steps = jnp.broadcast_to(step_ref[pl.ds(chunk, 1), :], (CHUNK, CHUNK))
    grid = jnp.round(steps * 8192.0) * (1.0 / 8192.0)

    def running(values):
        high, low = high_low(values)
        return dot_t(lower, high) + dot_t(lower, low)

    run = running(grid)
    coarse = jnp.round(run * 8.0) * 0.125
    fine = (run - coarse) + running(steps - grid)
    times_ref[0:1, :] += coarse[CHUNK - 1:]
    times_ref[1:2, :] += fine[CHUNK - 1:]
    elapsed = coarse + fine
    first = iota((CHUNK, LANES), 0) == 0
    for b in range(blocks):
        cols = slice(b * LANES, (b + 1) * LANES)
        rate = modes_ref[b:b + 1, :]
        freq = modes_ref[blocks + b:blocks + b + 1, :]
        cosine, sine = rotation(coarse, fine, split_turns(freq))
        exponent = rate * elapsed
        shrink = jnp.exp(-exponent)
        c_re[:, cols] = shrink * cosine
        c_im[:, cols] = shrink * sine
        grow = jnp.exp(exponent)
        g_re = grow * cosine
        g_im = -(grow * sine)
        d_re = jnp.where(first, 1.0, pltpu.roll(g_re, 1, 0)) - g_re
        d_im = jnp.where(first, 0.0, pltpu.roll(g_im, 1, 0)) - g_im
        scale = 1.0 / (rate * rate + freq * freq)
        l_re, l_im = -rate * scale, -freq * scale
        w_re[:, cols] = d_re * l_re - d_im * l_im
        w_im[:, cols] = d_re * l_im + d_im * l_re


def tables(step, rate, freq, input_map, readout):
    width = rate.size
    blocks = width // LANES
    chunks = step.shape[0]
    rows = chunks * CHUNK
    block = pl.BlockSpec((CHUNK, width), lambda c: (c, 0))
    big = jax.ShapeDtypeStruct((rows, width), F32)
    matrix = jax.ShapeDtypeStruct((blocks, 2 * LANES, 2 * LANES), BF16)
    modes = jax.ShapeDtypeStruct((2 * blocks, LANES), F32)
    times = jax.ShapeDtypeStruct((8, LANES), F32)
    small = [matrix, matrix, modes, times]
    return pl.pallas_call(
        tables_kernel, grid=(chunks,), in_specs=[whole(x) for x in (step, rate, freq, input_map, readout)],
        out_specs=[block] * 4 + [whole(x) for x in small], out_shape=[big] * 4 + small, name="tables",
        cost_estimate=pl.CostEstimate(flops=rows * width * 60, transcendentals=0, bytes_accessed=rows * width * 16),
    )(step, rate, freq, input_map, readout)


def project_kernel(at_ref, rows_ref, _, *refs):
    out_ref = refs[-1]
    ways = len(refs) - 1
    for back, proj in enumerate(refs[:-1]):
        owner = (at_ref[0] - back + ways) % ways
        out_ref[owner] = jnp.dot(rows_ref[...], proj[...], preferred_element_type=F32).astype(BF16)


def project(at, rows, after, projs):
    out = jax.ShapeDtypeStruct((len(projs), rows.shape[0], projs[0].shape[1]), BF16)
    return pl.pallas_call(
        project_kernel,
        grid_spec=pltpu.PrefetchScalarGridSpec(
            num_scalar_prefetch=1, grid=(1,), in_specs=[whole(x) for x in (rows, after, *projs)], out_specs=whole(out)),
        out_shape=out, name="project",
        cost_estimate=pl.CostEstimate(flops=2 * rows.size * len(projs) * LANES, transcendentals=0,
                                      bytes_accessed=4 * rows.size),
    )(at, rows, after, *projs)


def sums_kernel(drive_ref, w_re, w_im, c_re, c_im, push_ref, times_ref, acc_re, acc_im, sent_ref,
                stacked, carry):
    chunk = pl.program_id(0)
    blocks = push_ref.shape[0]

    @pl.when(chunk == 0)
    def _():
        carry[...] = jnp.zeros_like(carry)

    drive = drive_ref[...]
    twice = jnp.concatenate([drive, drive], axis=1)
    for b in range(blocks):
        cols = slice(b * LANES, (b + 1) * LANES)
        pushed = dot_t(twice, push_ref[b])
        p_re, p_im = pushed[:, :LANES], pushed[:, LANES:]
        wr, wi = w_re[:, cols], w_im[:, cols]
        high, low = high_low(wr * p_re - wi * p_im)
        stacked[b, :CHUNK, :LANES] = high
        stacked[b, CHUNK:, :LANES] = low
        high, low = high_low(wr * p_im + wi * p_re)
        stacked[b, :CHUNK, LANES:] = high
        stacked[b, CHUNK:, LANES:] = low
    lower = triangle(2)
    for b in range(blocks):
        cols = slice(b * LANES, (b + 1) * LANES)
        acc = jnp.dot(lower, stacked[b], preferred_element_type=F32)
        acc_re[:, cols] = acc[:, :LANES]
        acc_im[:, cols] = acc[:, LANES:]
        cr, ci = c_re[7:8, cols], c_im[7:8, cols]
        tr = acc[CHUNK - 1:, :LANES] + carry[b:b + 1, :]
        ti = acc[CHUNK - 1:, LANES:] + carry[blocks + b:blocks + b + 1, :]
        carry[b:b + 1, :] = cr * tr - ci * ti
        carry[blocks + b:blocks + b + 1, :] = cr * ti + ci * tr

    @pl.when(chunk == pl.num_programs(0) - 1)
    def _():
        message = jnp.concatenate([carry[...], times_ref[...]], axis=0)
        for k in range(sent_ref.shape[0]):
            sent_ref[k] = message


def sums(drive, w_re, w_im, c_re, c_im, push, times, peers):
    rows, width = w_re.shape
    blocks = width // LANES
    block = pl.BlockSpec((CHUNK, width), lambda c: (c, 0))
    last = pl.BlockSpec((8, width), lambda c: ((c + 1) * (CHUNK // 8) - 1, 0))
    big = jax.ShapeDtypeStruct((rows, width), F32)
    sent = jax.ShapeDtypeStruct((peers, 2 * blocks + 8, LANES), F32)
    return pl.pallas_call(
        sums_kernel, grid=(rows // CHUNK,),
        in_specs=[pl.BlockSpec((CHUNK, drive.shape[1]), lambda c: (c, 0)), block, block, last, last,
                  whole(push), whole(times)],
        out_specs=[block, block, whole(sent)],
        scratch_shapes=[pltpu.VMEM((blocks, 2 * CHUNK, 2 * LANES), BF16), pltpu.VMEM((2 * blocks, LANES), F32)],
        out_shape=[big, big, sent], name="sums",
        cost_estimate=pl.CostEstimate(flops=rows * width * 1500, transcendentals=0, bytes_accessed=rows * width * 16),
    )(drive, w_re, w_im, c_re, c_im, push, times)


def compose_kernel(at_ref, heard_ref, modes_ref, out_ref):
    blocks = modes_ref.shape[0] // 2
    rate = modes_ref[:blocks]
    turns = split_turns(modes_ref[blocks:])
    dr, di = jnp.ones(rate.shape, F32), jnp.zeros(rate.shape, F32)
    er, ei = jnp.zeros(rate.shape, F32), jnp.zeros(rate.shape, F32)
    count = heard_ref.shape[0]
    for k in range(count):
        @pl.when(at_ref[1] == k)
        def _(now=(er, ei, dr, di)):
            for j in range(4):
                out_ref[j * blocks:(j + 1) * blocks] = now[j]
        whole_time = heard_ref[k, 2 * blocks:2 * blocks + 1, :]
        coarse = jnp.round(whole_time)
        fine = (whole_time - coarse) + heard_ref[k, 2 * blocks + 1:2 * blocks + 2, :]
        xr, xi = decayed(coarse, fine, rate, turns)
        er, ei = (xr * er - xi * ei + heard_ref[k, :blocks], xr * ei + xi * er + heard_ref[k, blocks:2 * blocks])
        dr, di = xr * dr - xi * di, xr * di + xi * dr
    for j, value in enumerate((er, ei, dr, di)):
        out_ref[(4 + j) * blocks:(5 + j) * blocks] = value


def compose(at, heard, modes):
    out = jax.ShapeDtypeStruct((4 * modes.shape[0], LANES), F32)
    return pl.pallas_call(
        compose_kernel,
        grid_spec=pltpu.PrefetchScalarGridSpec(
            num_scalar_prefetch=1, grid=(1,), in_specs=[whole(heard), whole(modes)], out_specs=whole(out)),
        out_shape=out, name="compose",
    )(at, heard, modes)


def answer_kernel(near_ref, far_ref, acc_re, acc_im, c_re, c_im, read_ref, out_ref, high, low, carry):
    blocks = read_ref.shape[0]

    @pl.when(pl.program_id(0) == 0)
    def _():
        er, ei = near_ref[:blocks], near_ref[blocks:2 * blocks]
        dr, di = near_ref[2 * blocks:3 * blocks], near_ref[3 * blocks:4 * blocks]
        fr, fi = far_ref[:blocks], far_ref[blocks:]
        carry[:blocks] = dr * fr - di * fi + er
        carry[blocks:] = dr * fi + di * fr + ei

    for b in range(blocks):
        cols = slice(b * LANES, (b + 1) * LANES)
        tr = acc_re[:, cols] + carry[b:b + 1, :]
        ti = acc_im[:, cols] + carry[blocks + b:blocks + b + 1, :]
        cr, ci = c_re[:, cols], c_im[:, cols]
        sr = cr * tr - ci * ti
        si = cr * ti + ci * tr
        carry[b:b + 1, :] = sr[CHUNK - 1:]
        carry[blocks + b:blocks + b + 1, :] = si[CHUNK - 1:]
        high[b, :, :LANES], low[b, :, :LANES] = high_low(sr)
        high[b, :, LANES:], low[b, :, LANES:] = high_low(si)
    value = jnp.zeros((CHUNK, LANES), F32)
    for b in range(blocks):
        total = dot_t(high[b], read_ref[b])
        value = value + total[:, :LANES] + total[:, LANES:] + dot_t(low[b], read_ref[b, :LANES])
    inner = 0.7978845608 * (value + 0.044715 * (value * value * value))
    out_ref[...] = (0.5 * value * (1.0 + jnp.tanh(inner))).astype(BF16)


def answers(near, far, acc_re, acc_im, c_re, c_im, read):
    rows, width = acc_re.shape
    blocks = width // LANES
    block = pl.BlockSpec((CHUNK, width), lambda c: (c, 0))
    store = pltpu.VMEM((blocks, CHUNK, 2 * LANES), BF16)
    return pl.pallas_call(
        answer_kernel, grid=(rows // CHUNK,),
        in_specs=[whole(near), whole(far)] + [block] * 4 + [whole(read)],
        out_specs=pl.BlockSpec((CHUNK, LANES), lambda c: (c, 0)),
        scratch_shapes=[store, store, pltpu.VMEM((2 * blocks, LANES), F32)],
        out_shape=jax.ShapeDtypeStruct((rows, LANES), BF16), name="answers",
        cost_estimate=pl.CostEstimate(flops=rows * width * 1000, transcendentals=0, bytes_accessed=rows * width * 16),
    )(near, far, acc_re, acc_im, c_re, c_im, read)


def output_kernel(parts_ref, gain_ref, proj_ref, out_ref, shaped):
    pieces, _, part = parts_ref.shape

    @pl.when(pl.program_id(0) == 0)
    def _():
        total = jnp.zeros((parts_ref.shape[1], 1), F32)
        for k in range(pieces):
            values = parts_ref[k].astype(F32)
            total = total + jnp.sum(values * values, axis=1, keepdims=True)
        factor = lax.rsqrt(total * (1.0 / (pieces * part)) + 1e-06)
        for k in range(pieces):
            cols = slice(k * part, (k + 1) * part)
            shaped[:, cols] = (parts_ref[k].astype(F32) * factor * gain_ref[:, cols]).astype(BF16)

    out_ref[...] = jnp.dot(shaped[...], proj_ref[...], preferred_element_type=F32).astype(BF16)


def output(parts, gain, proj, tile=512):
    rows = parts.shape[1]
    width = proj.shape[1]
    return pl.pallas_call(
        output_kernel, grid=(width // tile,),
        in_specs=[whole(parts), whole(gain), pl.BlockSpec((proj.shape[0], tile), lambda n: (0, n))],
        out_specs=pl.BlockSpec((rows, tile), lambda n: (0, n)),
        scratch_shapes=[pltpu.VMEM((rows, proj.shape[0]), BF16)],
        out_shape=jax.ShapeDtypeStruct((rows, width), BF16), name="output",
    )(parts, gain, proj)


def rms_rows(values, gain):
    values = values.astype(F32)
    scaled = values * lax.rsqrt(jnp.mean(values * values, axis=-1, keepdims=True) + 1e-06)
    return (scaled * gain).astype(BF16)


def ring(count, by):
    return [(k, (k + by) % count) for k in range(count)]


def on_device(
    tokens, step, in_gain, in_proj, decay_rate, frequency, input_map, readout, out_gain, out_proj
):
    ways = lax.axis_size("tp")
    place = lax.axis_index(("zl", "core"))
    at = jnp.stack([lax.axis_index("tp"), place]).astype(jnp.int32)
    projs = [in_proj] + [lax.ppermute(in_proj, "tp", ring(ways, by)) for by in range(1, ways)]
    w_re, w_im, c_re, c_im, push, read, modes, times = tables(
        step.reshape(-1, CHUNK), decay_rate, frequency, input_map, readout
    )
    normed = rms_rows(tokens, in_gain)
    drive = lax.all_to_all(project(at, normed, times, projs), "tp", 0, 0, tiled=True)
    peers = lax.axis_size("zl") * lax.axis_size("core")
    acc_re, acc_im, sent = sums(
        drive.reshape(-1, drive.shape[-1]), w_re, w_im, c_re, c_im, push, times, peers
    )
    near = compose(at, lax.all_to_all(sent, ("zl", "core"), 0, 0, tiled=True), modes)
    half = modes.shape[0]
    quarter = half // 2
    er, ei, dr, di = (near[2 * half + k * quarter:2 * half + (k + 1) * quarter] for k in range(4))
    fr = jnp.zeros_like(er)
    fi = jnp.zeros_like(ei)
    for k in range(lax.axis_size("zh") - 1):
        leaves = jnp.concatenate([dr * fr - di * fi + er, dr * fi + di * fr + ei], axis=0)
        comes = lax.ppermute(leaves, "zh", [(k, k + 1)])
        fr, fi = fr + comes[:quarter], fi + comes[quarter:]
    far = jnp.concatenate([fr, fi], axis=0)
    answer = answers(near, far, acc_re, acc_im, c_re, c_im, read)
    parts = lax.all_to_all(answer.reshape(ways, -1, LANES), "tp", 0, 0, tiled=True)
    return output(parts, out_gain.reshape(1, -1), out_proj)


def solution(mesh):
    shape = mesh.shape
    chips = shape["sp"] // 2
    near = min(BLOCK, chips)
    devices = mesh.devices.reshape(shape["grp"], chips // near, near, 2, shape["tp"])
    fine_mesh = Mesh(devices, ("grp", "zh", "zl", "core", "tp"))
    rows = ("grp", "zh", "zl", "core", "tp")
    placed = (
        P(rows, None),
        P(("grp", "zh", "zl", "core")),
        P(),
        P(None, "tp"),
        P("tp", None),
        P("tp", None),
        P(None, "tp", None, None),
        P(None, "tp", None, None),
        P(),
        P(),
    )
    return jax.shard_map(
        on_device,
        mesh=fine_mesh,
        in_specs=placed,
        out_specs=P(rows, None),
        check_vma=False,
    )
```

```python
from functools import partial

import jax
import jax.numpy as jnp
from jax import lax
from jax.experimental import pallas as pl
from jax.experimental.pallas import tpu as pltpu
from jax.sharding import Mesh, PartitionSpec as P

CHUNK = 128
TILE = 512
LANES = 128
BLOCK = 4
F32 = jnp.float32
BF16 = jnp.bfloat16
TWO_PI_HIGH = 6.28125
TWO_PI_LOW = 0.0019353071795864769
INV_TWO_PI = 0.15915494309189535
SIN = (6.2831854820251465, -41.3416862487793, 81.60456085205078, -76.69428253173828,
       41.96574020385742, -14.708574295043945, 3.0096182823181152)
COS = (1.0, -19.739208221435547, 64.9393539428711, -85.45588684082031, 60.23442077636719,
       -26.364990234375, 7.6985273361206055, -1.3503994941711426)


def polynomial(x, factors):
    total = factors[-1] * x + factors[-2]
    for factor in factors[-3::-1]:
        total = total * x + factor
    return total


def split_turns(freq):
    plain = freq * INV_TWO_PI
    high = jnp.round(plain * 8192.0) * (1.0 / 8192.0)
    rest = (freq - high * TWO_PI_HIGH) - high * TWO_PI_LOW
    return high, rest * INV_TWO_PI, plain


def rotation(coarse, fine, turns, again=False):
    high, rest, plain = turns
    whole = coarse * high
    part = (whole - jnp.round(whole)) + (coarse * rest + fine * plain)
    if again:
        part = part - jnp.round(part)
    square = part * part
    return polynomial(square, COS), part * polynomial(square, SIN)


def decayed(coarse, fine, rate, turns):
    cosine, sine = rotation(coarse, fine, turns, again=True)
    magnitude = jnp.exp(-rate * (coarse + fine))
    return magnitude * cosine, magnitude * sine


def high_low(x):
    high = x.astype(BF16)
    return high, (x - high.astype(F32)).astype(BF16)


def dot_t(a, b):
    return lax.dot_general(a, b, (((1,), (1,)), ((), ())), preferred_element_type=F32)


def whole(array):
    return pl.BlockSpec(array.shape, lambda *at: (0,) * array.ndim)


def iota(shape, dim):
    return lax.broadcasted_iota(jnp.int32, shape, dim)


def triangle(repeat=1):
    shape = (CHUNK, repeat * CHUNK)
    return jnp.where((iota(shape, 1) % CHUNK) <= iota(shape, 0), 1.0, 0.0).astype(BF16)


def selection(shape, shift):
    return jnp.where(iota(shape, 1) == iota(shape, 0) + shift, 1.0, 0.0).astype(BF16)


def moved(rows, piece, cols):
    kept = dot_t(rows, piece).astype(BF16)
    return jnp.dot(kept, cols, preferred_element_type=F32)


def tables_kernel(tokens_ref, gain_ref, step_ref, rate_ref, freq_ref, map_ref, readout_ref,
                  normed_ref, w_re, w_im, c_re, c_im,
                  end_re, end_im, push_ref, read_ref, modes_ref, times_ref):
    chunk = pl.program_id(0)
    blocks = modes_ref.shape[0] // 2
    per_block, entries = rate_ref.shape[0] // blocks, rate_ref.shape[1]

    @pl.when(chunk == 0)
    def _():
        times_ref[...] = jnp.zeros_like(times_ref)
        for b in range(blocks):
            mine = range(per_block * b, per_block * (b + 1))
            modes_ref[b:b + 1, :] = jnp.concatenate([rate_ref[g:g + 1, :] for g in mine], axis=1)
            modes_ref[blocks + b:blocks + b + 1, :] = jnp.concatenate([freq_ref[g:g + 1, :] for g in mine], axis=1)

    for b in range(blocks):
        @pl.when(chunk == b)
        def _(b=b):
            members = map_ref.shape[2]
            for part in range(2):
                sign = 1.0 if part == 0 else -1.0
                pushes, reads = [0.0, 0.0], [0.0, 0.0]
                for j in range(per_block):
                    g = per_block * b + j
                    seat = selection((entries, LANES), entries * j)
                    seat_t = selection((LANES, entries), -entries * j)
                    place = selection((members, LANES), members * g)
                    place_t = selection((LANES, members), -members * g)
                    for k, piece in enumerate(high_low(map_ref[part, g])):
                        kept = jnp.dot(place_t, piece, preferred_element_type=F32).astype(BF16)
                        pushes[k] = pushes[k] + jnp.dot(kept, seat, preferred_element_type=F32)
                    for k, piece in enumerate(high_low(sign * readout_ref[part, g])):
                        reads[k] = reads[k] + moved(seat_t, piece, place)
                for k in range(2):
                    push_ref[b, k * LANES:(k + 1) * LANES, part * LANES:(part + 1) * LANES] = pushes[k].astype(BF16)
                    read_ref[b, part * LANES:(part + 1) * LANES, k * LANES:(k + 1) * LANES] = reads[k].astype(BF16)

    tokens = tokens_ref[...].astype(F32)
    mean = jnp.mean(tokens * tokens, axis=1, keepdims=True)
    normed_ref[...] = (tokens * lax.rsqrt(mean + 1e-06) * gain_ref[...]).astype(BF16)

    lower = triangle()
    steps = jnp.broadcast_to(step_ref[pl.ds(chunk, 1), :], (CHUNK, CHUNK))
    grid = jnp.round(steps * 8192.0) * (1.0 / 8192.0)

    def running(values):
        high, low = high_low(values)
        return dot_t(lower, high) + dot_t(lower, low)

    run = running(grid)
    coarse = jnp.round(run * 8.0) * 0.125
    fine = (run - coarse) + running(steps - grid)
    times_ref[0:1, :] += coarse[CHUNK - 1:]
    times_ref[1:2, :] += fine[CHUNK - 1:]
    elapsed = coarse + fine
    first = iota((CHUNK, LANES), 0) == 0
    for b in range(blocks):
        cols = slice(b * LANES, (b + 1) * LANES)
        rate = modes_ref[b:b + 1, :]
        freq = modes_ref[blocks + b:blocks + b + 1, :]
        cosine, sine = rotation(coarse, fine, split_turns(freq))
        exponent = rate * elapsed
        shrink = jnp.exp(-exponent)
        c_re[:, cols] = shrink * cosine
        c_im[:, cols] = shrink * sine
        end_re[:, cols] = (shrink * cosine)[CHUNK - 8:]
        end_im[:, cols] = (shrink * sine)[CHUNK - 8:]
        grow = jnp.exp(exponent)
        g_re = grow * cosine
        g_im = -(grow * sine)
        d_re = jnp.where(first, 1.0, pltpu.roll(g_re, 1, 0)) - g_re
        d_im = jnp.where(first, 0.0, pltpu.roll(g_im, 1, 0)) - g_im
        scale = 1.0 / (rate * rate + freq * freq)
        l_re, l_im = -rate * scale, -freq * scale
        w_re[:, cols] = d_re * l_re - d_im * l_im
        w_im[:, cols] = d_re * l_im + d_im * l_re


def tables(tokens, gain, step, rate, freq, input_map, readout):
    width = rate.size
    blocks = width // LANES
    chunks = step.shape[0]
    rows = chunks * CHUNK
    part = pl.BlockSpec((tokens.shape[0] // chunks, tokens.shape[1]), lambda c: (c, 0))
    block = pl.BlockSpec((CHUNK, width), lambda c: (c, 0))
    big = jax.ShapeDtypeStruct((rows, width), F32)
    end = jax.ShapeDtypeStruct((8 * chunks, width), F32)
    last = pl.BlockSpec((8, width), lambda c: (c, 0))
    matrix = jax.ShapeDtypeStruct((blocks, 2 * LANES, 2 * LANES), BF16)
    modes = jax.ShapeDtypeStruct((2 * blocks, LANES), F32)
    times = jax.ShapeDtypeStruct((8, LANES), F32)
    small = [matrix, matrix, modes, times]
    return pl.pallas_call(
        tables_kernel, grid=(chunks,),
        in_specs=[part, whole(gain)] + [whole(x) for x in (step, rate, freq, input_map, readout)],
        out_specs=[part] + [block] * 4 + [last] * 2 + [whole(x) for x in small], out_shape=[jax.ShapeDtypeStruct(tokens.shape, BF16)] + [big] * 4 + [end] * 2 + small, name="tables",
        cost_estimate=pl.CostEstimate(flops=rows * width * 60, transcendentals=0, bytes_accessed=rows * width * 16),
    )(tokens, gain, step, rate, freq, input_map, readout)


def project_kernel(at_ref, rows_ref, *refs):
    *projs, out_ref = refs
    ways = len(projs)
    width = projs[0].shape[1]
    rows = rows_ref[...]
    for back in range(0, ways, 2):
        pair = jnp.concatenate([projs[back][...], projs[back + 1][...]], axis=1)
        both = jnp.dot(rows, pair, preferred_element_type=F32).astype(BF16)
        for k in range(2):
            out_ref[(at_ref[0] - back - k + ways) % ways] = both[:, k * width:(k + 1) * width]


def project(at, rows, projs, tile=256):
    width = projs[0].shape[1]
    out = jax.ShapeDtypeStruct((len(projs), rows.shape[0], width), BF16)
    return pl.pallas_call(
        project_kernel,
        grid_spec=pltpu.PrefetchScalarGridSpec(
            num_scalar_prefetch=1, grid=(rows.shape[0] // tile,),
            in_specs=[pl.BlockSpec((tile, rows.shape[1]), lambda k, at: (k, 0))]
            + [whole(x) for x in projs],
            out_specs=pl.BlockSpec((len(projs), tile, width), lambda k, at: (0, k, 0))),
        out_shape=out, name="project",
        cost_estimate=pl.CostEstimate(flops=2 * rows.size * len(projs) * width, transcendentals=0,
                                      bytes_accessed=4 * rows.size),
    )(at, rows, *projs)


def ends_kernel(drive_ref, w_re, w_im, c_re, c_im, push_ref, times_ref, stacked, sent_ref, carry):
    chunk = pl.program_id(0)
    blocks = push_ref.shape[0]

    @pl.when(chunk == 0)
    def _():
        carry[...] = jnp.zeros_like(carry)

    drive = drive_ref[...]
    twice = jnp.concatenate([drive, drive], axis=1)
    for b in range(blocks):
        cols = slice(b * LANES, (b + 1) * LANES)
        pushed = jnp.dot(twice, push_ref[b], preferred_element_type=F32)
        er, ei = carry[b:b + 1, :], carry[blocks + b:blocks + b + 1, :]
        for k in range(TILE // CHUNK):
            rows = slice(k * CHUNK, (k + 1) * CHUNK)
            p_re, p_im = pushed[rows, :LANES], pushed[rows, LANES:]
            wr, wi = w_re[rows, cols], w_im[rows, cols]
            x_re = wr * p_re - wi * p_im
            x_im = wr * p_im + wi * p_re
            stacked[k, b, :CHUNK, :LANES], stacked[k, b, CHUNK:, :LANES] = high_low(x_re)
            stacked[k, b, :CHUNK, LANES:], stacked[k, b, CHUNK:, LANES:] = high_low(x_im)
            last = 8 * k + 7
            cr, ci = c_re[last:last + 1, cols], c_im[last:last + 1, cols]
            tr = jnp.sum(x_re, axis=0, keepdims=True) + er
            ti = jnp.sum(x_im, axis=0, keepdims=True) + ei
            er, ei = cr * tr - ci * ti, cr * ti + ci * tr
        carry[b:b + 1, :] = er
        carry[blocks + b:blocks + b + 1, :] = ei

    @pl.when(chunk == pl.num_programs(0) - 1)
    def _():
        message = jnp.concatenate([carry[...], times_ref[...]], axis=0)
        for k in range(sent_ref.shape[0]):
            sent_ref[k] = message


def ends(drive, w_re, w_im, d_re, d_im, push, times, peers):
    rows, width = w_re.shape
    blocks = width // LANES
    chunks = TILE // CHUNK
    block = pl.BlockSpec((TILE, width), lambda c: (c, 0))
    last = pl.BlockSpec((8 * chunks, width), lambda c: (c, 0))
    stacked = jax.ShapeDtypeStruct((rows // CHUNK, blocks, 2 * CHUNK, 2 * LANES), BF16)
    sent = jax.ShapeDtypeStruct((peers, 2 * blocks + 8, LANES), F32)
    return pl.pallas_call(
        ends_kernel, grid=(rows // TILE,),
        in_specs=[pl.BlockSpec((TILE, drive.shape[1]), lambda c: (c, 0)), block, block, last, last,
                  whole(push), whole(times)],
        out_specs=[pl.BlockSpec((chunks, *stacked.shape[1:]), lambda c: (c, 0, 0, 0)), whole(sent)],
        scratch_shapes=[pltpu.VMEM((2 * blocks, LANES), F32)],
        out_shape=[stacked, sent], name="ends",
        cost_estimate=pl.CostEstimate(flops=rows * width * 500, transcendentals=0, bytes_accessed=rows * width * 16),
    )(drive, w_re, w_im, d_re, d_im, push, times)


def read_states(high, low, read):
    total = jnp.dot(high, read, preferred_element_type=F32)
    return total[:, :LANES] + total[:, LANES:] + jnp.dot(low, read[:, :LANES], preferred_element_type=F32)


def local_kernel(stacked, c_re, c_im, read_ref, out_ref, high, low, carry):
    blocks = read_ref.shape[0]

    @pl.when(pl.program_id(0) == 0)
    def _():
        carry[...] = jnp.zeros_like(carry)

    lower = triangle(2)
    for b in range(blocks):
        cols = slice(b * LANES, (b + 1) * LANES)
        er, ei = carry[b:b + 1, :], carry[blocks + b:blocks + b + 1, :]
        for k in range(TILE // CHUNK):
            rows = slice(k * CHUNK, (k + 1) * CHUNK)
            acc = jnp.dot(lower, stacked[k, b], preferred_element_type=F32)
            tr, ti = acc[:, :LANES] + er, acc[:, LANES:] + ei
            cr, ci = c_re[rows, cols], c_im[rows, cols]
            sr = cr * tr - ci * ti
            si = cr * ti + ci * tr
            er, ei = sr[CHUNK - 1:], si[CHUNK - 1:]
            high[b, rows, :LANES], low[b, rows, :LANES] = high_low(sr)
            high[b, rows, LANES:], low[b, rows, LANES:] = high_low(si)
        carry[b:b + 1, :] = er
        carry[blocks + b:blocks + b + 1, :] = ei
    value = jnp.zeros((TILE, LANES), F32)
    for b in range(blocks):
        value = value + read_states(high[b], low[b], read_ref[b])
    out_ref[...] = value


def scratches(blocks):
    store = pltpu.VMEM((blocks, TILE, 2 * LANES), BF16)
    return [store, store, pltpu.VMEM((2 * blocks, LANES), F32)]


def local(stacked, c_re, c_im, read):
    rows, width = c_re.shape
    block = pl.BlockSpec((TILE, width), lambda c: (c, 0))
    return pl.pallas_call(
        local_kernel, grid=(rows // TILE,),
        in_specs=[pl.BlockSpec((TILE // CHUNK, *stacked.shape[1:]), lambda c: (c, 0, 0, 0)), block, block, whole(read)],
        out_specs=pl.BlockSpec((TILE, LANES), lambda c: (c, 0)),
        scratch_shapes=scratches(width // LANES),
        out_shape=jax.ShapeDtypeStruct((rows, LANES), F32), name="local",
        cost_estimate=pl.CostEstimate(flops=rows * width * 1500, transcendentals=0, bytes_accessed=rows * width * 16),
    )(stacked, c_re, c_im, read)


def compose_kernel(at_ref, heard_ref, modes_ref, _, out_ref):
    blocks = modes_ref.shape[0] // 2
    rate = modes_ref[:blocks]
    turns = split_turns(modes_ref[blocks:])
    dr, di = jnp.ones(rate.shape, F32), jnp.zeros(rate.shape, F32)
    er, ei = jnp.zeros(rate.shape, F32), jnp.zeros(rate.shape, F32)
    near = (er, ei, dr, di)
    for k in range(heard_ref.shape[0]):
        near = [jnp.where(at_ref[1] == k, new, old) for new, old in zip((er, ei, dr, di), near)]
        whole_time = heard_ref[k, 2 * blocks:2 * blocks + 1, :]
        coarse = jnp.round(whole_time)
        fine = (whole_time - coarse) + heard_ref[k, 2 * blocks + 1:2 * blocks + 2, :]
        xr, xi = decayed(coarse, fine, rate, turns)
        er, ei = (xr * er - xi * ei + heard_ref[k, :blocks], xr * ei + xi * er + heard_ref[k, blocks:2 * blocks])
        dr, di = xr * dr - xi * di, xr * di + xi * dr
    for j, value in enumerate(near):
        out_ref[j * blocks:(j + 1) * blocks] = value
    for j, value in enumerate((er, ei, dr, di)):
        out_ref[(4 + j) * blocks:(5 + j) * blocks] = value


def compose(at, heard, modes, after):
    out = jax.ShapeDtypeStruct((4 * modes.shape[0], LANES), F32)
    return pl.pallas_call(
        compose_kernel,
        grid_spec=pltpu.PrefetchScalarGridSpec(
            num_scalar_prefetch=1, grid=(1,), in_specs=[whole(heard), whole(modes), pl.BlockSpec((8, LANES), lambda c, at: (0, 0))],
            out_specs=whole(out)),
        out_shape=out, name="compose",
    )(at, heard, modes, after)


def answer_kernel(near_ref, far_ref, local_ref, c_re, c_im, read_ref, out_ref, high, low, carry):
    blocks = read_ref.shape[0]

    @pl.when(pl.program_id(0) == 0)
    def _():
        er, ei = near_ref[:blocks], near_ref[blocks:2 * blocks]
        dr, di = near_ref[2 * blocks:3 * blocks], near_ref[3 * blocks:4 * blocks]
        fr, fi = far_ref[:blocks], far_ref[blocks:]
        carry[:blocks] = dr * fr - di * fi + er
        carry[blocks:] = dr * fi + di * fr + ei

    for b in range(blocks):
        cols = slice(b * LANES, (b + 1) * LANES)
        er, ei = carry[b:b + 1, :], carry[blocks + b:blocks + b + 1, :]
        for k in range(TILE // CHUNK):
            rows = slice(k * CHUNK, (k + 1) * CHUNK)
            cr, ci = c_re[rows, cols], c_im[rows, cols]
            sr = cr * er - ci * ei
            si = cr * ei + ci * er
            er, ei = sr[CHUNK - 1:], si[CHUNK - 1:]
            high[b, rows, :LANES], low[b, rows, :LANES] = high_low(sr)
            high[b, rows, LANES:], low[b, rows, LANES:] = high_low(si)
        carry[b:b + 1, :] = er
        carry[blocks + b:blocks + b + 1, :] = ei
    value = local_ref[...]
    for b in range(blocks):
        value = value + read_states(high[b], low[b], read_ref[b])
    inner = 0.7978845608 * (value + 0.044715 * (value * value * value))
    out_ref[...] = (0.5 * value * (1.0 + jnp.tanh(inner))).astype(BF16)


def answers(near, far, locals_, c_re, c_im, read):
    rows, width = c_re.shape
    block = pl.BlockSpec((TILE, width), lambda c: (c, 0))
    narrow = pl.BlockSpec((TILE, LANES), lambda c: (c, 0))
    return pl.pallas_call(
        answer_kernel, grid=(rows // TILE,),
        in_specs=[whole(near), whole(far), narrow, block, block, whole(read)],
        out_specs=narrow, scratch_shapes=scratches(width // LANES),
        out_shape=jax.ShapeDtypeStruct((rows, LANES), BF16), name="answers",
        cost_estimate=pl.CostEstimate(flops=rows * width * 1000, transcendentals=0, bytes_accessed=rows * width * 16),
    )(near, far, locals_, c_re, c_im, read)


def ring(count, by):
    return [(k, (k + by) % count) for k in range(count)]


def on_device(
    tokens, step, in_gain, in_proj, decay_rate, frequency, input_map, readout, out_gain, out_proj
):
    ways = lax.axis_size("tp")
    place = lax.axis_index(("zl", "core"))
    at = jnp.stack([lax.axis_index("tp"), place]).astype(jnp.int32)
    projs = [in_proj] + [lax.ppermute(in_proj, "tp", ring(ways, by)) for by in range(1, ways)]
    normed, w_re, w_im, c_re, c_im, d_re, d_im, push, read, modes, times = tables(
        tokens, in_gain.reshape(1, -1), step.reshape(-1, CHUNK), decay_rate, frequency,
        jnp.swapaxes(input_map, 2, 3), readout,
    )
    drive = lax.all_to_all(project(at, normed, projs), "tp", 0, 0, tiled=True)
    peers = lax.axis_size("zl") * lax.axis_size("core")
    stacked, sent = ends(
        drive.reshape(-1, drive.shape[-1]), w_re, w_im, d_re, d_im, push, times, peers
    )
    heard = lax.all_to_all(sent, ("zl", "core"), 0, 0, tiled=True)
    own = local(stacked, c_re, c_im, read)
    near = compose(at, heard, modes, own)
    half = modes.shape[0]
    quarter = half // 2
    er, ei, dr, di = (near[2 * half + k * quarter:2 * half + (k + 1) * quarter] for k in range(4))
    er, ei, dr, di = lax.optimization_barrier((er, ei, dr, di))
    fr = jnp.zeros_like(er)
    fi = jnp.zeros_like(ei)
    for k in range(lax.axis_size("zh") - 1):
        leaves = jnp.concatenate([dr * fr - di * fi + er, dr * fi + di * fr + ei], axis=0)
        comes = lax.ppermute(leaves, "zh", [(k, k + 1)])
        fr, fi = fr + comes[:quarter], fi + comes[quarter:]
    far = jnp.concatenate([fr, fi], axis=0)
    answer = answers(near, far, own, c_re, c_im, read)
    parts = lax.all_to_all(answer.reshape(ways, -1, LANES), "tp", 0, 0, tiled=True)
    values = parts.astype(F32)
    mean = jnp.sum(values * values, axis=(0, 2), keepdims=True) * (1.0 / (ways * LANES))
    shaped = (values * lax.rsqrt(mean + 1e-06) * out_gain.reshape(ways, 1, LANES)).astype(BF16)
    return jnp.einsum(
        "ktc,kcd->td", shaped, out_proj.reshape(ways, LANES, -1), preferred_element_type=F32
    ).astype(BF16)


def solution(mesh):
    shape = mesh.shape
    chips = shape["sp"] // 2
    near = min(BLOCK, chips)
    devices = mesh.devices.reshape(shape["grp"], chips // near, near, 2, shape["tp"])
    fine_mesh = Mesh(devices, ("grp", "zh", "zl", "core", "tp"))
    rows = ("grp", "zh", "zl", "core", "tp")
    placed = (
        P(rows, None),
        P(("grp", "zh", "zl", "core")),
        P(),
        P(None, "tp"),
        P("tp", None),
        P("tp", None),
        P(None, "tp", None, None),
        P(None, "tp", None, None),
        P(),
        P(),
    )
    return jax.shard_map(
        on_device,
        mesh=fine_mesh,
        in_specs=placed,
        out_specs=P(rows, None),
        check_vma=False,
    )
```

```python
from functools import partial

import jax
import jax.numpy as jnp
from jax import lax
from jax.experimental import pallas as pl
from jax.experimental.pallas import tpu as pltpu
from jax.sharding import Mesh, PartitionSpec as P

CHUNK = 128
TILE = 1024
GRANT = 24 * 1024 * 1024
LANES = 128
BLOCK = 4
F32 = jnp.float32
BF16 = jnp.bfloat16
TWO_PI_HIGH = 6.28125
TWO_PI_LOW = 0.0019353071795864769
INV_TWO_PI = 0.15915494309189535
SIN = (6.2831854820251465, -41.3416862487793, 81.60456085205078, -76.69428253173828,
       41.96574020385742, -14.708574295043945, 3.0096182823181152)
COS = (1.0, -19.739208221435547, 64.9393539428711, -85.45588684082031, 60.23442077636719,
       -26.364990234375, 7.6985273361206055, -1.3503994941711426)


def polynomial(x, factors):
    total = factors[-1] * x + factors[-2]
    for factor in factors[-3::-1]:
        total = total * x + factor
    return total


def split_turns(freq):
    plain = freq * INV_TWO_PI
    high = jnp.round(plain * 8192.0) * (1.0 / 8192.0)
    rest = (freq - high * TWO_PI_HIGH) - high * TWO_PI_LOW
    return high, rest * INV_TWO_PI, plain


def rotation(coarse, fine, turns, again=False):
    high, rest, plain = turns
    whole = coarse * high
    part = (whole - jnp.round(whole)) + (coarse * rest + fine * plain)
    if again:
        part = part - jnp.round(part)
    square = part * part
    return polynomial(square, COS), part * polynomial(square, SIN)


def decayed(coarse, fine, rate, turns):
    cosine, sine = rotation(coarse, fine, turns, again=True)
    magnitude = jnp.exp(-rate * (coarse + fine))
    return magnitude * cosine, magnitude * sine


def high_low(x):
    high = x.astype(BF16)
    return high, (x - high.astype(F32)).astype(BF16)


def dot_t(a, b):
    return lax.dot_general(a, b, (((1,), (1,)), ((), ())), preferred_element_type=F32)


def whole(array):
    return pl.BlockSpec(array.shape, lambda *at: (0,) * array.ndim)


ONCHIP = pl.BlockSpec(memory_space=pltpu.VMEM)


def onchip(x):
    return pltpu.with_memory_space_constraint(x, pltpu.VMEM)


def settings():
    return pltpu.CompilerParams(vmem_limit_bytes=GRANT)


def iota(shape, dim):
    return lax.broadcasted_iota(jnp.int32, shape, dim)


def triangle(repeat=1):
    shape = (CHUNK, repeat * CHUNK)
    return jnp.where((iota(shape, 1) % CHUNK) <= iota(shape, 0), 1.0, 0.0).astype(BF16)


def selection(shape, shift):
    return jnp.where(iota(shape, 1) == iota(shape, 0) + shift, 1.0, 0.0).astype(BF16)


def moved(rows, piece, cols):
    kept = jnp.dot(rows, piece, preferred_element_type=F32).astype(BF16)
    return jnp.dot(kept, cols, preferred_element_type=F32)


def tables_kernel(tokens_ref, gain_ref, step_ref, rate_ref, freq_ref, map_ref, readout_ref,
                  normed_ref, w_re, w_im, c_re, c_im,
                  end_re, end_im, push_ref, read_ref, modes_ref, times_ref, ready):
    chunk = pl.program_id(0)
    blocks = modes_ref.shape[0] // 2
    per_block, entries = rate_ref.shape[0] // blocks, rate_ref.shape[1]

    @pl.when(chunk == 0)
    def _():
        times_ref[...] = jnp.zeros_like(times_ref)
        for b in range(blocks):
            mine = range(per_block * b, per_block * (b + 1))
            modes_ref[b:b + 1, :] = jnp.concatenate([rate_ref[g:g + 1, :] for g in mine], axis=1)
            modes_ref[blocks + b:blocks + b + 1, :] = jnp.concatenate([freq_ref[g:g + 1, :] for g in mine], axis=1)

    block, part = chunk // 2, chunk % 2
    members = map_ref.shape[2]
    sign = (1 - 2 * part).astype(F32)
    pushes, reads = [0.0, 0.0], [0.0, 0.0]
    for j in range(per_block):
        g = per_block * block + j
        seat = selection((entries, LANES), entries * j)
        seat_t = selection((LANES, entries), -entries * j)
        place = selection((members, LANES), members * g)
        place_t = selection((LANES, members), -members * g)
        for k, piece in enumerate(high_low(map_ref[part, g])):
            pushes[k] = pushes[k] + moved(place_t, piece, seat)
        for k, piece in enumerate(high_low(sign * readout_ref[part, g])):
            kept = dot_t(seat_t, piece).astype(BF16)
            reads[k] = reads[k] + jnp.dot(kept, place, preferred_element_type=F32)
    for k in range(2):
        push_ref[block, part, k * LANES:(k + 1) * LANES, :] = pushes[k].astype(BF16)
        read_ref[block, part, :, k * LANES:(k + 1) * LANES] = reads[k].astype(BF16)

    tokens = tokens_ref[...].astype(F32)
    mean = jnp.mean(tokens * tokens, axis=1, keepdims=True)
    share = tokens.shape[0]
    normed_ref[pl.ds(pl.multiple_of(chunk * share, share), share), :] = (tokens * lax.rsqrt(mean + 1e-06) * gain_ref[...]).astype(BF16)

    lower = iota((CHUNK, CHUNK), 1) <= iota((CHUNK, CHUNK), 0)
    ones = jnp.ones((2 * CHUNK, LANES), BF16)

    def running(values):
        kept = [jnp.where(lower, x.astype(F32), 0.0).astype(BF16) for x in high_low(values)]
        return jnp.dot(jnp.concatenate(kept, axis=1), ones, preferred_element_type=F32)

    def timed(which):
        steps = jnp.broadcast_to(step_ref[pl.ds(which, 1), :], (CHUNK, CHUNK))
        grid = jnp.round(steps * 8192.0) * (1.0 / 8192.0)
        run = running(grid)
        coarse = jnp.round(run * 8.0) * 0.125
        return coarse, (run - coarse) + running(steps - grid)

    @pl.when(chunk == 0)
    def _():
        ready[0, 0], ready[0, 1] = timed(0)

    now = pl.ds(pl.multiple_of(chunk * CHUNK, CHUNK), CHUNK)
    end = pl.ds(pl.multiple_of(chunk * 8, 8), 8)
    coarse, fine = ready[chunk % 2, 0], ready[chunk % 2, 1]
    following = timed(jnp.minimum(chunk + 1, pl.num_programs(0) - 1))
    times_ref[0:1, :] += coarse[CHUNK - 1:]
    times_ref[1:2, :] += fine[CHUNK - 1:]
    elapsed = coarse + fine
    first = iota((CHUNK, LANES), 0) == 0
    for b in range(blocks):
        cols = slice(b * LANES, (b + 1) * LANES)
        rate = modes_ref[b:b + 1, :]
        freq = modes_ref[blocks + b:blocks + b + 1, :]
        cosine, sine = rotation(coarse, fine, split_turns(freq))
        exponent = rate * elapsed
        shrink = jnp.exp(-exponent)
        c_re[now, cols] = shrink * cosine
        c_im[now, cols] = shrink * sine
        end_re[end, cols] = (shrink * cosine)[CHUNK - 8:]
        end_im[end, cols] = (shrink * sine)[CHUNK - 8:]
        grow = jnp.exp(exponent)
        g_re = grow * cosine
        g_im = -(grow * sine)
        d_re = jnp.where(first, 1.0, pltpu.roll(g_re, 1, 0)) - g_re
        d_im = jnp.where(first, 0.0, pltpu.roll(g_im, 1, 0)) - g_im
        scale = 1.0 / (rate * rate + freq * freq)
        l_re, l_im = -rate * scale, -freq * scale
        w_re[now, cols] = d_re * l_re - d_im * l_im
        w_im[now, cols] = d_re * l_im + d_im * l_re
    ready[(chunk + 1) % 2, 0], ready[(chunk + 1) % 2, 1] = following


def tables(tokens, gain, step, rate, freq, input_map, readout):
    width = rate.size
    blocks = width // LANES
    chunks = step.shape[0]
    rows = chunks * CHUNK
    part = pl.BlockSpec((tokens.shape[0] // chunks, tokens.shape[1]), lambda c: (c, 0))
    out = [pltpu.VMEM(tokens.shape, BF16)] + [pltpu.VMEM((rows, width), F32)] * 4
    out += [pltpu.VMEM((8 * chunks, width), F32)] * 2
    out += [pltpu.VMEM((blocks, 2, 2 * LANES, LANES), BF16), pltpu.VMEM((blocks, 2, LANES, 2 * LANES), BF16)]
    out += [pltpu.VMEM((2 * blocks, LANES), F32), pltpu.VMEM((8, LANES), F32)]
    return pl.pallas_call(
        tables_kernel, grid=(chunks,),
        in_specs=[part, whole(gain)] + [whole(x) for x in (step, rate, freq, input_map, readout)],
        out_specs=[ONCHIP] * len(out), out_shape=out, name="tables", compiler_params=settings(),
        scratch_shapes=[pltpu.VMEM((2, 2, CHUNK, LANES), F32)],
        cost_estimate=pl.CostEstimate(flops=rows * width * 60, transcendentals=0, bytes_accessed=rows * width * 16),
    )(*(pltpu.with_memory_space_constraint(x, pltpu.HBM) for x in (tokens, gain, step, rate, freq, input_map, readout)))


def project_kernel(at_ref, rows_ref, *refs):
    *projs, out_ref = refs
    ways = len(projs)
    width = projs[0].shape[1]
    rows = rows_ref[...]
    for back in range(0, ways, 2):
        pair = jnp.concatenate([projs[back][...], projs[back + 1][...]], axis=1)
        both = jnp.dot(rows, pair, preferred_element_type=F32).astype(BF16)
        for k in range(2):
            out_ref[(at_ref[0] - back - k + ways) % ways] = both[:, k * width:(k + 1) * width]


def project(at, rows, projs):
    width = projs[0].shape[1]
    return pl.pallas_call(
        project_kernel,
        grid_spec=pltpu.PrefetchScalarGridSpec(
            num_scalar_prefetch=1, grid=(1,), in_specs=[ONCHIP] * (1 + len(projs)), out_specs=ONCHIP),
        out_shape=pltpu.VMEM((len(projs), rows.shape[0], width), BF16), name="project", compiler_params=settings(),
        cost_estimate=pl.CostEstimate(flops=2 * rows.size * len(projs) * width, transcendentals=0,
                                      bytes_accessed=4 * rows.size),
    )(at, onchip(rows), *(onchip(x) for x in projs))


def ends_kernel(drive_ref, w_re, w_im, d_re, d_im, push_ref, times_ref, stacked, sent_ref):
    blocks = push_ref.shape[0]
    tiles = drive_ref.shape[0] // TILE
    ends_re, ends_im = [], []
    for b in range(blocks):
        cols = slice(b * LANES, (b + 1) * LANES)
        push = jnp.concatenate([push_ref[b, 0], push_ref[b, 1]], axis=1)
        er = ei = jnp.zeros((1, LANES), F32)
        for tile in range(tiles):
            drive = drive_ref[tile * TILE:(tile + 1) * TILE, :]
            pushed = jnp.dot(jnp.concatenate([drive, drive], axis=1), push, preferred_element_type=F32)
            for j in range(TILE // CHUNK):
                k = tile * (TILE // CHUNK) + j
                rows = slice(k * CHUNK, (k + 1) * CHUNK)
                part = pushed[j * CHUNK:(j + 1) * CHUNK]
                p_re, p_im = part[:, :LANES], part[:, LANES:]
                wr, wi = w_re[rows, cols], w_im[rows, cols]
                x_re = wr * p_re - wi * p_im
                x_im = wr * p_im + wi * p_re
                stacked[k, b, :CHUNK, :LANES], stacked[k, b, CHUNK:, :LANES] = high_low(x_re)
                stacked[k, b, :CHUNK, LANES:], stacked[k, b, CHUNK:, LANES:] = high_low(x_im)
                last = 8 * k + 7
                cr, ci = d_re[last:last + 1, cols], d_im[last:last + 1, cols]
                tr = jnp.sum(x_re, axis=0, keepdims=True) + er
                ti = jnp.sum(x_im, axis=0, keepdims=True) + ei
                er, ei = cr * tr - ci * ti, cr * ti + ci * tr
        ends_re.append(er)
        ends_im.append(ei)
    message = jnp.concatenate(ends_re + ends_im + [times_ref[...]], axis=0)
    for k in range(sent_ref.shape[0]):
        sent_ref[k] = message


def ends(drive, w_re, w_im, d_re, d_im, push, times, peers):
    rows, width = w_re.shape
    blocks = width // LANES
    return pl.pallas_call(
        ends_kernel, in_specs=[ONCHIP] * 7, out_specs=[ONCHIP] * 2, compiler_params=settings(),
        out_shape=[pltpu.VMEM((rows // CHUNK, blocks, 2 * CHUNK, 2 * LANES), BF16),
                   pltpu.VMEM((peers, 2 * blocks + 8, LANES), F32)], name="ends",
        cost_estimate=pl.CostEstimate(flops=rows * width * 500, transcendentals=0, bytes_accessed=rows * width * 16),
    )(*(onchip(x) for x in (drive, w_re, w_im, d_re, d_im, push, times)))


def read_states(high, low, read):
    total = jnp.dot(high, read, preferred_element_type=F32)
    return total[:, :LANES] + total[:, LANES:] + jnp.dot(low, read[:, :LANES], preferred_element_type=F32)


def read_of(read_ref, b):
    return jnp.concatenate([read_ref[b, 0], read_ref[b, 1]], axis=0)


def local_kernel(stacked, c_re, c_im, read_ref, _, out_ref, high, low):
    blocks = read_ref.shape[0]
    lower = triangle(2)
    carry = [jnp.zeros((1, LANES), F32)] * (2 * blocks)
    for tile in range(c_re.shape[0] // TILE):
        value = jnp.zeros((TILE, LANES), F32)
        for b in range(blocks):
            cols = slice(b * LANES, (b + 1) * LANES)
            er, ei = carry[2 * b:2 * b + 2]
            for j in range(TILE // CHUNK):
                k = tile * (TILE // CHUNK) + j
                rows = slice(k * CHUNK, (k + 1) * CHUNK)
                here = slice(j * CHUNK, (j + 1) * CHUNK)
                acc = jnp.dot(lower, stacked[k, b], preferred_element_type=F32)
                tr, ti = acc[:, :LANES] + er, acc[:, LANES:] + ei
                cr, ci = c_re[rows, cols], c_im[rows, cols]
                sr = cr * tr - ci * ti
                si = cr * ti + ci * tr
                er, ei = sr[CHUNK - 1:], si[CHUNK - 1:]
                high[b, here, :LANES], low[b, here, :LANES] = high_low(sr)
                high[b, here, LANES:], low[b, here, LANES:] = high_low(si)
            carry[2 * b], carry[2 * b + 1] = er, ei
        for b in range(blocks):
            value = value + read_states(high[b], low[b], read_of(read_ref, b))
        out_ref[tile * TILE:(tile + 1) * TILE, :] = value


def scratches(blocks):
    store = pltpu.VMEM((blocks, TILE, 2 * LANES), BF16)
    return [store, store]


def local(stacked, c_re, c_im, read, after):
    rows, width = c_re.shape
    return pl.pallas_call(
        local_kernel, in_specs=[ONCHIP] * 5, out_specs=ONCHIP, scratch_shapes=scratches(width // LANES),
        out_shape=pltpu.VMEM((rows, LANES), F32), name="local", compiler_params=settings(),
        cost_estimate=pl.CostEstimate(flops=rows * width * 1500, transcendentals=0, bytes_accessed=rows * width * 16),
    )(*(onchip(x) for x in (stacked, c_re, c_im, read, after)))


def compose_kernel(at_ref, heard_ref, modes_ref, out_ref, end_ref, decay_ref):
    blocks = modes_ref.shape[0] // 2
    rate = modes_ref[:blocks]
    turns = split_turns(modes_ref[blocks:])
    dr, di = jnp.ones(rate.shape, F32), jnp.zeros(rate.shape, F32)
    er, ei = jnp.zeros(rate.shape, F32), jnp.zeros(rate.shape, F32)
    near = (er, ei, dr, di)
    for k in range(heard_ref.shape[0]):
        near = [jnp.where(at_ref[0] == k, new, old) for new, old in zip((er, ei, dr, di), near)]
        whole_time = heard_ref[k, 2 * blocks:2 * blocks + 1, :]
        coarse = jnp.round(whole_time)
        fine = (whole_time - coarse) + heard_ref[k, 2 * blocks + 1:2 * blocks + 2, :]
        xr, xi = decayed(coarse, fine, rate, turns)
        er, ei = (xr * er - xi * ei + heard_ref[k, :blocks], xr * ei + xi * er + heard_ref[k, blocks:2 * blocks])
        dr, di = xr * dr - xi * di, xr * di + xi * dr
    for j, value in enumerate(near):
        out_ref[j * blocks:(j + 1) * blocks] = value
    end_ref[:blocks], end_ref[blocks:] = er, ei
    decay_ref[:blocks], decay_ref[blocks:] = dr, di


def compose(at, heard, modes):
    one = pltpu.VMEM(modes.shape, F32)
    return pl.pallas_call(
        compose_kernel,
        grid_spec=pltpu.PrefetchScalarGridSpec(
            num_scalar_prefetch=1, grid=(1,), in_specs=[ONCHIP] * 2, out_specs=[ONCHIP] * 3),
        out_shape=[pltpu.VMEM((2 * modes.shape[0], LANES), F32), one, one], name="compose",
        compiler_params=settings(),
    )(at, *(onchip(x) for x in (heard, modes)))


def link_kernel(far_ref, comes_ref, end_ref, decay_ref, next_ref, leaves_ref):
    blocks = far_ref.shape[0] // 2
    far = far_ref[...] + comes_ref[...]
    fr, fi = far[:blocks], far[blocks:]
    dr, di = decay_ref[:blocks], decay_ref[blocks:]
    next_ref[...] = far
    leaves_ref[...] = end_ref[...] + jnp.concatenate([dr * fr - di * fi, dr * fi + di * fr], axis=0)


def link(far, comes, end, decay):
    out = pltpu.VMEM(far.shape, F32)
    return pl.pallas_call(
        link_kernel, in_specs=[ONCHIP] * 4, out_specs=[ONCHIP] * 2, out_shape=[out, out], name="link",
        compiler_params=settings(),
    )(*(onchip(x) for x in (far, comes, end, decay)))


def answer_kernel(near_ref, far_ref, local_ref, c_re, c_im, d_re, d_im, read_ref, out_ref, high, low):
    blocks = read_ref.shape[0]
    er, ei = near_ref[:blocks], near_ref[blocks:2 * blocks]
    dr, di = near_ref[2 * blocks:3 * blocks], near_ref[3 * blocks:4 * blocks]
    fr, fi = far_ref[:blocks], far_ref[blocks:]
    start_re = dr * fr - di * fi + er
    start_im = dr * fi + di * fr + ei
    carry = [x[b:b + 1] for b in range(blocks) for x in (start_re, start_im)]
    for tile in range(c_re.shape[0] // TILE):
        for b in range(blocks):
            cols = slice(b * LANES, (b + 1) * LANES)
            er, ei = carry[2 * b:2 * b + 2]
            for j in range(TILE // CHUNK):
                k = tile * (TILE // CHUNK) + j
                rows = slice(k * CHUNK, (k + 1) * CHUNK)
                here = slice(j * CHUNK, (j + 1) * CHUNK)
                cr, ci = c_re[rows, cols], c_im[rows, cols]
                sr = cr * er - ci * ei
                si = cr * ei + ci * er
                high[b, here, :LANES], low[b, here, :LANES] = high_low(sr)
                high[b, here, LANES:], low[b, here, LANES:] = high_low(si)
                last = 8 * k + 7
                cr, ci = d_re[last:last + 1, cols], d_im[last:last + 1, cols]
                er, ei = cr * er - ci * ei, cr * ei + ci * er
            carry[2 * b], carry[2 * b + 1] = er, ei
        value = local_ref[tile * TILE:(tile + 1) * TILE, :]
        for b in range(blocks):
            value = value + read_states(high[b], low[b], read_of(read_ref, b))
        inner = 0.7978845608 * (value + 0.044715 * (value * value * value))
        out_ref[tile * TILE:(tile + 1) * TILE, :] = (0.5 * value * (1.0 + jnp.tanh(inner))).astype(BF16)


def answers(near, far, own, c_re, c_im, d_re, d_im, read):
    rows, width = c_re.shape
    return pl.pallas_call(
        answer_kernel, in_specs=[ONCHIP] * 8, out_specs=ONCHIP, scratch_shapes=scratches(width // LANES),
        out_shape=pltpu.VMEM((rows, LANES), BF16), name="answers", compiler_params=settings(),
        cost_estimate=pl.CostEstimate(flops=rows * width * 1000, transcendentals=0, bytes_accessed=rows * width * 16),
    )(*(onchip(x) for x in (near, far, own, c_re, c_im, d_re, d_im, read)))


def ring(count, by):
    return [(k, (k + by) % count) for k in range(count)]


def on_device(
    tokens, step, in_gain, in_proj, decay_rate, frequency, input_map, readout, out_gain, out_proj
):
    ways = lax.axis_size("tp")
    way = lax.axis_index("tp").astype(jnp.int32).reshape(1)
    place = lax.axis_index(("zl", "core")).astype(jnp.int32).reshape(1)
    step, way, place = lax.optimization_barrier((step, way, place))
    projs = [in_proj] + [lax.ppermute(in_proj, "tp", ring(ways, by)) for by in range(1, ways)]
    normed, w_re, w_im, c_re, c_im, d_re, d_im, push, read, modes, times = tables(
        tokens, in_gain.reshape(1, -1), step.reshape(-1, CHUNK), decay_rate, frequency,
        jnp.swapaxes(input_map, 2, 3), readout,
    )
    drive = lax.all_to_all(project(way, normed, projs), "tp", 0, 0, tiled=True)
    peers = lax.axis_size("zl") * lax.axis_size("core")
    stacked, sent = ends(
        drive.reshape(-1, drive.shape[-1]), w_re, w_im, d_re, d_im, push, times, peers
    )
    heard = lax.all_to_all(sent, ("zl", "core"), 0, 0, tiled=True)
    own = local(stacked, c_re, c_im, read, heard)
    near, end, decay = compose(place, heard, modes)
    far, leaves = jnp.zeros_like(end), end
    for k in range(lax.axis_size("zh") - 1):
        comes = lax.ppermute(leaves, "zh", [(k, k + 1)])
        far, leaves = link(far, comes, end, decay)
    answer = answers(near, far, own, c_re, c_im, d_re, d_im, read)
    parts = lax.all_to_all(answer.reshape(ways, -1, LANES), "tp", 0, 0, tiled=True)
    values = parts.astype(F32)
    mean = jnp.sum(values * values, axis=(0, 2), keepdims=True) * (1.0 / (ways * LANES))
    shaped = (values * lax.rsqrt(mean + 1e-06) * out_gain.reshape(ways, 1, LANES)).astype(BF16)
    return jnp.einsum(
        "ktc,kcd->td", shaped, out_proj.reshape(ways, LANES, -1), preferred_element_type=F32
    ).astype(BF16)


def solution(mesh):
    shape = mesh.shape
    chips = shape["sp"] // 2
    near = min(BLOCK, chips)
    devices = mesh.devices.reshape(shape["grp"], chips // near, near, 2, shape["tp"])
    fine_mesh = Mesh(devices, ("grp", "zh", "zl", "core", "tp"))
    rows = ("grp", "zh", "zl", "core", "tp")
    placed = (
        P(rows, None),
        P(("grp", "zh", "zl", "core")),
        P(),
        P(None, "tp"),
        P("tp", None),
        P("tp", None),
        P(None, "tp", None, None),
        P(None, "tp", None, None),
        P(),
        P(),
    )
    return jax.shard_map(
        on_device,
        mesh=fine_mesh,
        in_specs=placed,
        out_specs=P(rows, None),
        check_vma=False,
    )
```

```python
from functools import partial

import jax
import jax.numpy as jnp
from jax import lax
from jax.experimental import pallas as pl
from jax.experimental.pallas import tpu as pltpu
from jax.sharding import Mesh, PartitionSpec as P

CHUNK = 128
TILE = 1024
GRANT = 24 * 1024 * 1024
LANES = 128
BLOCK = 4
F32 = jnp.float32
BF16 = jnp.bfloat16
TWO_PI_HIGH = 6.28125
TWO_PI_LOW = 0.0019353071795864769
INV_TWO_PI = 0.15915494309189535
SIN = (6.2831854820251465, -41.3416862487793, 81.60456085205078, -76.69428253173828,
       41.96574020385742, -14.708574295043945, 3.0096182823181152)
COS = (1.0, -19.739208221435547, 64.9393539428711, -85.45588684082031, 60.23442077636719,
       -26.364990234375, 7.6985273361206055, -1.3503994941711426)


def polynomial(x, factors):
    total = factors[-1] * x + factors[-2]
    for factor in factors[-3::-1]:
        total = total * x + factor
    return total


def split_turns(freq):
    plain = freq * INV_TWO_PI
    high = jnp.round(plain * 8192.0) * (1.0 / 8192.0)
    rest = (freq - high * TWO_PI_HIGH) - high * TWO_PI_LOW
    return high, rest * INV_TWO_PI, plain


def rotation(coarse, fine, turns, again=False):
    high, rest, plain = turns
    whole = coarse * high
    part = (whole - jnp.round(whole)) + (coarse * rest + fine * plain)
    if again:
        part = part - jnp.round(part)
    square = part * part
    return polynomial(square, COS), part * polynomial(square, SIN)


def decayed(coarse, fine, rate, turns):
    cosine, sine = rotation(coarse, fine, turns, again=True)
    magnitude = jnp.exp(-rate * (coarse + fine))
    return magnitude * cosine, magnitude * sine


def high_low(x):
    high = x.astype(BF16)
    return high, (x - high.astype(F32)).astype(BF16)


def dot_t(a, b):
    return lax.dot_general(a, b, (((1,), (1,)), ((), ())), preferred_element_type=F32)


def whole(array):
    return pl.BlockSpec(array.shape, lambda *at: (0,) * array.ndim)


ONCHIP = pl.BlockSpec(memory_space=pltpu.VMEM)


def onchip(x):
    return pltpu.with_memory_space_constraint(x, pltpu.VMEM)


def settings():
    return pltpu.CompilerParams(vmem_limit_bytes=GRANT)


def iota(shape, dim):
    return lax.broadcasted_iota(jnp.int32, shape, dim)


def triangle(repeat=1):
    shape = (CHUNK, repeat * CHUNK)
    return jnp.where((iota(shape, 1) % CHUNK) <= iota(shape, 0), 1.0, 0.0).astype(BF16)


def selection(shape, shift):
    return jnp.where(iota(shape, 1) == iota(shape, 0) + shift, 1.0, 0.0).astype(BF16)


def moved(rows, piece, cols):
    kept = jnp.dot(rows, piece, preferred_element_type=F32).astype(BF16)
    return jnp.dot(kept, cols, preferred_element_type=F32)


def tables_kernel(tokens_ref, proj_ref, gain_ref, step_ref, rate_ref, freq_ref, map_ref, readout_ref,
                  normed_ref, kept_ref, w_re, w_im, c_re, c_im,
                  end_re, end_im, push_ref, read_ref, modes_ref, times_ref, ready):
    chunk = pl.program_id(0)
    blocks = modes_ref.shape[0] // 2
    per_block, entries = rate_ref.shape[0] // blocks, rate_ref.shape[1]

    @pl.when(chunk == 0)
    def _():
        times_ref[...] = jnp.zeros_like(times_ref)
        for b in range(blocks):
            mine = range(per_block * b, per_block * (b + 1))
            modes_ref[b:b + 1, :] = jnp.concatenate([rate_ref[g:g + 1, :] for g in mine], axis=1)
            modes_ref[blocks + b:blocks + b + 1, :] = jnp.concatenate([freq_ref[g:g + 1, :] for g in mine], axis=1)

    block, part = chunk // 2, chunk % 2
    members = map_ref.shape[2]
    sign = (1 - 2 * part).astype(F32)
    pushes, reads = [0.0, 0.0], [0.0, 0.0]
    for j in range(per_block):
        g = per_block * block + j
        seat = selection((entries, LANES), entries * j)
        seat_t = selection((LANES, entries), -entries * j)
        place = selection((members, LANES), members * g)
        place_t = selection((LANES, members), -members * g)
        for k, piece in enumerate(high_low(map_ref[part, g])):
            pushes[k] = pushes[k] + moved(place_t, piece, seat)
        for k, piece in enumerate(high_low(sign * readout_ref[part, g])):
            kept = dot_t(seat_t, piece).astype(BF16)
            reads[k] = reads[k] + jnp.dot(kept, place, preferred_element_type=F32)
    for k in range(2):
        push_ref[block, part, k * LANES:(k + 1) * LANES, :] = pushes[k].astype(BF16)
        read_ref[block, part, :, k * LANES:(k + 1) * LANES] = reads[k].astype(BF16)

    tokens = tokens_ref[...].astype(F32)
    mean = jnp.mean(tokens * tokens, axis=1, keepdims=True)
    share = tokens.shape[0]
    normed_ref[pl.ds(pl.multiple_of(chunk * share, share), share), :] = (tokens * lax.rsqrt(mean + 1e-06) * gain_ref[...]).astype(BF16)

    deep = proj_ref.shape[0]
    kept_ref[pl.ds(pl.multiple_of(chunk * deep, deep), deep), :] = proj_ref[...]

    lower = iota((CHUNK, CHUNK), 1) <= iota((CHUNK, CHUNK), 0)
    ones = jnp.ones((2 * CHUNK, LANES), BF16)

    def running(values):
        kept = [jnp.where(lower, x.astype(F32), 0.0).astype(BF16) for x in high_low(values)]
        return jnp.dot(jnp.concatenate(kept, axis=1), ones, preferred_element_type=F32)

    def timed(which):
        steps = jnp.broadcast_to(step_ref[pl.ds(which, 1), :], (CHUNK, CHUNK))
        grid = jnp.round(steps * 8192.0) * (1.0 / 8192.0)
        run = running(grid)
        coarse = jnp.round(run * 8.0) * 0.125
        return coarse, (run - coarse) + running(steps - grid)

    @pl.when(chunk == 0)
    def _():
        ready[0, 0], ready[0, 1] = timed(0)

    now = pl.ds(pl.multiple_of(chunk * CHUNK, CHUNK), CHUNK)
    end = pl.ds(pl.multiple_of(chunk * 8, 8), 8)
    coarse, fine = ready[chunk % 2, 0], ready[chunk % 2, 1]
    following = timed(jnp.minimum(chunk + 1, pl.num_programs(0) - 1))
    times_ref[0:1, :] += coarse[CHUNK - 1:]
    times_ref[1:2, :] += fine[CHUNK - 1:]
    elapsed = coarse + fine
    first = iota((CHUNK, LANES), 0) == 0
    for b in range(blocks):
        cols = slice(b * LANES, (b + 1) * LANES)
        rate = modes_ref[b:b + 1, :]
        freq = modes_ref[blocks + b:blocks + b + 1, :]
        cosine, sine = rotation(coarse, fine, split_turns(freq))
        exponent = rate * elapsed
        shrink = jnp.exp(-exponent)
        c_re[now, cols] = shrink * cosine
        c_im[now, cols] = shrink * sine
        end_re[end, cols] = (shrink * cosine)[CHUNK - 8:]
        end_im[end, cols] = (shrink * sine)[CHUNK - 8:]
        grow = jnp.exp(exponent)
        g_re = grow * cosine
        g_im = -(grow * sine)
        d_re = jnp.where(first, 1.0, pltpu.roll(g_re, 1, 0)) - g_re
        d_im = jnp.where(first, 0.0, pltpu.roll(g_im, 1, 0)) - g_im
        scale = 1.0 / (rate * rate + freq * freq)
        l_re, l_im = -rate * scale, -freq * scale
        w_re[now, cols] = d_re * l_re - d_im * l_im
        w_im[now, cols] = d_re * l_im + d_im * l_re
    ready[(chunk + 1) % 2, 0], ready[(chunk + 1) % 2, 1] = following


def tables(tokens, proj, gain, step, rate, freq, input_map, readout):
    width = rate.size
    blocks = width // LANES
    chunks = step.shape[0]
    rows = chunks * CHUNK
    part = pl.BlockSpec((tokens.shape[0] // chunks, tokens.shape[1]), lambda c: (c, 0))
    slab = pl.BlockSpec((proj.shape[0] // chunks, proj.shape[1]), lambda c: (c, 0))
    out = [pltpu.VMEM(tokens.shape, BF16), pltpu.VMEM(proj.shape, BF16)] + [pltpu.VMEM((rows, width), F32)] * 4
    out += [pltpu.VMEM((8 * chunks, width), F32)] * 2
    out += [pltpu.VMEM((blocks, 2, 2 * LANES, LANES), BF16), pltpu.VMEM((blocks, 2, LANES, 2 * LANES), BF16)]
    out += [pltpu.VMEM((2 * blocks, LANES), F32), pltpu.VMEM((8, LANES), F32)]
    return pl.pallas_call(
        tables_kernel, grid=(chunks,),
        in_specs=[part, slab, whole(gain)] + [whole(x) for x in (step, rate, freq, input_map, readout)],
        out_specs=[ONCHIP] * len(out), out_shape=out, name="tables", compiler_params=settings(),
        scratch_shapes=[pltpu.VMEM((2, 2, CHUNK, LANES), F32)],
        cost_estimate=pl.CostEstimate(flops=rows * width * 60, transcendentals=0, bytes_accessed=rows * width * 16),
    )(*(pltpu.with_memory_space_constraint(x, pltpu.HBM) for x in (tokens, proj, gain, step, rate, freq, input_map, readout)))


def project_kernel(at_ref, rows_ref, *refs):
    *projs, out_ref = refs
    ways = len(projs)
    width = projs[0].shape[1]
    rows = rows_ref[...]
    for back in range(0, ways, 2):
        pair = jnp.concatenate([projs[back][...], projs[back + 1][...]], axis=1)
        both = jnp.dot(rows, pair, preferred_element_type=F32).astype(BF16)
        for k in range(2):
            out_ref[(at_ref[0] - back - k + ways) % ways] = both[:, k * width:(k + 1) * width]


def project(at, rows, projs):
    width = projs[0].shape[1]
    return pl.pallas_call(
        project_kernel,
        grid_spec=pltpu.PrefetchScalarGridSpec(
            num_scalar_prefetch=1, grid=(1,), in_specs=[ONCHIP] * (1 + len(projs)), out_specs=ONCHIP),
        out_shape=pltpu.VMEM((len(projs), rows.shape[0], width), BF16), name="project", compiler_params=settings(),
        cost_estimate=pl.CostEstimate(flops=2 * rows.size * len(projs) * width, transcendentals=0,
                                      bytes_accessed=4 * rows.size),
    )(at, onchip(rows), *(onchip(x) for x in projs))


def ends_kernel(drive_ref, w_re, w_im, d_re, d_im, push_ref, times_ref, stacked, sent_ref):
    blocks = push_ref.shape[0]
    tiles = drive_ref.shape[0] // TILE
    ends_re, ends_im = [], []
    for b in range(blocks):
        cols = slice(b * LANES, (b + 1) * LANES)
        push = jnp.concatenate([push_ref[b, 0], push_ref[b, 1]], axis=1)
        er = ei = jnp.zeros((1, LANES), F32)
        for tile in range(tiles):
            drive = drive_ref[tile * TILE:(tile + 1) * TILE, :]
            pushed = jnp.dot(jnp.concatenate([drive, drive], axis=1), push, preferred_element_type=F32)
            for j in range(TILE // CHUNK):
                k = tile * (TILE // CHUNK) + j
                rows = slice(k * CHUNK, (k + 1) * CHUNK)
                part = pushed[j * CHUNK:(j + 1) * CHUNK]
                p_re, p_im = part[:, :LANES], part[:, LANES:]
                wr, wi = w_re[rows, cols], w_im[rows, cols]
                x_re = wr * p_re - wi * p_im
                x_im = wr * p_im + wi * p_re
                stacked[k, b, :CHUNK, :LANES], stacked[k, b, CHUNK:, :LANES] = high_low(x_re)
                stacked[k, b, :CHUNK, LANES:], stacked[k, b, CHUNK:, LANES:] = high_low(x_im)
                last = 8 * k + 7
                cr, ci = d_re[last:last + 1, cols], d_im[last:last + 1, cols]
                tr = jnp.sum(x_re, axis=0, keepdims=True) + er
                ti = jnp.sum(x_im, axis=0, keepdims=True) + ei
                er, ei = cr * tr - ci * ti, cr * ti + ci * tr
        ends_re.append(er)
        ends_im.append(ei)
    message = jnp.concatenate(ends_re + ends_im + [times_ref[...]], axis=0)
    for k in range(sent_ref.shape[0]):
        sent_ref[k] = message


def ends(drive, w_re, w_im, d_re, d_im, push, times, peers):
    rows, width = w_re.shape
    blocks = width // LANES
    return pl.pallas_call(
        ends_kernel, in_specs=[ONCHIP] * 7, out_specs=[ONCHIP] * 2, compiler_params=settings(),
        out_shape=[pltpu.VMEM((rows // CHUNK, blocks, 2 * CHUNK, 2 * LANES), BF16),
                   pltpu.VMEM((peers, 2 * blocks + 8, LANES), F32)], name="ends",
        cost_estimate=pl.CostEstimate(flops=rows * width * 500, transcendentals=0, bytes_accessed=rows * width * 16),
    )(*(onchip(x) for x in (drive, w_re, w_im, d_re, d_im, push, times)))


def read_states(high, low, read):
    total = jnp.dot(high, read, preferred_element_type=F32)
    return total[:, :LANES] + total[:, LANES:] + jnp.dot(low, read[:, :LANES], preferred_element_type=F32)


def read_of(read_ref, b):
    return jnp.concatenate([read_ref[b, 0], read_ref[b, 1]], axis=0)


def scratches(blocks):
    store = pltpu.VMEM((blocks, TILE, 2 * LANES), BF16)
    return [store, store]


def compose_kernel(at_ref, heard_ref, modes_ref, out_ref, end_ref, decay_ref):
    blocks = modes_ref.shape[0] // 2
    rate = modes_ref[:blocks]
    turns = split_turns(modes_ref[blocks:])
    dr, di = jnp.ones(rate.shape, F32), jnp.zeros(rate.shape, F32)
    er, ei = jnp.zeros(rate.shape, F32), jnp.zeros(rate.shape, F32)
    near = (er, ei, dr, di)
    for k in range(heard_ref.shape[0]):
        near = [jnp.where(at_ref[0] == k, new, old) for new, old in zip((er, ei, dr, di), near)]
        whole_time = heard_ref[k, 2 * blocks:2 * blocks + 1, :]
        coarse = jnp.round(whole_time)
        fine = (whole_time - coarse) + heard_ref[k, 2 * blocks + 1:2 * blocks + 2, :]
        xr, xi = decayed(coarse, fine, rate, turns)
        er, ei = (xr * er - xi * ei + heard_ref[k, :blocks], xr * ei + xi * er + heard_ref[k, blocks:2 * blocks])
        dr, di = xr * dr - xi * di, xr * di + xi * dr
    for j, value in enumerate(near):
        out_ref[j * blocks:(j + 1) * blocks] = value
    end_ref[:blocks], end_ref[blocks:] = er, ei
    decay_ref[:blocks], decay_ref[blocks:] = dr, di


def compose(at, heard, modes):
    one = pltpu.VMEM(modes.shape, F32)
    return pl.pallas_call(
        compose_kernel,
        grid_spec=pltpu.PrefetchScalarGridSpec(
            num_scalar_prefetch=1, grid=(1,), in_specs=[ONCHIP] * 2, out_specs=[ONCHIP] * 3),
        out_shape=[pltpu.VMEM((2 * modes.shape[0], LANES), F32), one, one], name="compose",
        compiler_params=settings(),
    )(at, *(onchip(x) for x in (heard, modes)))


def link_kernel(far_ref, comes_ref, end_ref, decay_ref, next_ref, leaves_ref):
    blocks = far_ref.shape[0] // 2
    far = far_ref[...] + comes_ref[...]
    fr, fi = far[:blocks], far[blocks:]
    dr, di = decay_ref[:blocks], decay_ref[blocks:]
    next_ref[...] = far
    leaves_ref[...] = end_ref[...] + jnp.concatenate([dr * fr - di * fi, dr * fi + di * fr], axis=0)


def link(far, comes, end, decay):
    out = pltpu.VMEM(far.shape, F32)
    return pl.pallas_call(
        link_kernel, in_specs=[ONCHIP] * 4, out_specs=[ONCHIP] * 2, out_shape=[out, out], name="link",
        compiler_params=settings(),
    )(*(onchip(x) for x in (far, comes, end, decay)))


def answer_kernel(near_ref, far_ref, comes_ref, stacked, c_re, c_im, read_ref, out_ref, high, low):
    blocks = read_ref.shape[0]
    er, ei = near_ref[:blocks], near_ref[blocks:2 * blocks]
    dr, di = near_ref[2 * blocks:3 * blocks], near_ref[3 * blocks:4 * blocks]
    far = far_ref[...] + comes_ref[...]
    fr, fi = far[:blocks], far[blocks:]
    start_re = dr * fr - di * fi + er
    start_im = dr * fi + di * fr + ei
    carry = [x[b:b + 1] for b in range(blocks) for x in (start_re, start_im)]
    lower = triangle(2)
    for tile in range(c_re.shape[0] // TILE):
        for b in range(blocks):
            cols = slice(b * LANES, (b + 1) * LANES)
            er, ei = carry[2 * b:2 * b + 2]
            for j in range(TILE // CHUNK):
                k = tile * (TILE // CHUNK) + j
                rows = slice(k * CHUNK, (k + 1) * CHUNK)
                here = slice(j * CHUNK, (j + 1) * CHUNK)
                acc = jnp.dot(lower, stacked[k, b], preferred_element_type=F32)
                tr, ti = acc[:, :LANES] + er, acc[:, LANES:] + ei
                cr, ci = c_re[rows, cols], c_im[rows, cols]
                sr = cr * tr - ci * ti
                si = cr * ti + ci * tr
                er, ei = sr[CHUNK - 1:], si[CHUNK - 1:]
                high[b, here, :LANES], low[b, here, :LANES] = high_low(sr)
                high[b, here, LANES:], low[b, here, LANES:] = high_low(si)
            carry[2 * b], carry[2 * b + 1] = er, ei
        value = jnp.zeros((TILE, LANES), F32)
        for b in range(blocks):
            value = value + read_states(high[b], low[b], read_of(read_ref, b))
        inner = 0.7978845608 * (value + 0.044715 * (value * value * value))
        out_ref[tile * TILE:(tile + 1) * TILE, :] = (0.5 * value * (1.0 + jnp.tanh(inner))).astype(BF16)


def answers(near, far, comes, stacked, c_re, c_im, read):
    rows, width = c_re.shape
    return pl.pallas_call(
        answer_kernel, in_specs=[ONCHIP] * 7, out_specs=ONCHIP, scratch_shapes=scratches(width // LANES),
        out_shape=pltpu.VMEM((rows, LANES), BF16), name="answers", compiler_params=settings(),
        cost_estimate=pl.CostEstimate(flops=rows * width * 1500, transcendentals=0, bytes_accessed=rows * width * 16),
    )(*(onchip(x) for x in (near, far, comes, stacked, c_re, c_im, read)))


def ring(count, by):
    return [(k, (k + by) % count) for k in range(count)]


def on_device(
    tokens, step, in_gain, in_proj, decay_rate, frequency, input_map, readout, out_gain, out_proj
):
    ways = lax.axis_size("tp")
    way = lax.axis_index("tp").astype(jnp.int32).reshape(1)
    place = lax.axis_index(("zl", "core")).astype(jnp.int32).reshape(1)
    step, way, place = lax.optimization_barrier((step, way, place))
    projs = [lax.ppermute(in_proj, "tp", ring(ways, by)) for by in range(1, ways)]
    normed, kept, w_re, w_im, c_re, c_im, d_re, d_im, push, read, modes, times = tables(
        tokens, in_proj, in_gain.reshape(1, -1), step.reshape(-1, CHUNK), decay_rate, frequency,
        jnp.swapaxes(input_map, 2, 3), readout,
    )
    drive = lax.all_to_all(project(way, normed, [kept, *projs]), "tp", 0, 0, tiled=True)
    peers = lax.axis_size("zl") * lax.axis_size("core")
    stacked, sent = ends(
        drive.reshape(-1, drive.shape[-1]), w_re, w_im, d_re, d_im, push, times, peers
    )
    heard = lax.all_to_all(sent, ("zl", "core"), 0, 0, tiled=True)
    near, end, decay = compose(place, heard, modes)
    far, comes, leaves = jnp.zeros_like(end), jnp.zeros_like(end), end
    steps = lax.axis_size("zh") - 1
    for k in range(steps):
        comes = lax.ppermute(leaves, "zh", [(k, k + 1)])
        if k < steps - 1:
            far, leaves = link(far, comes, end, decay)
    answer = answers(near, far, comes, stacked, c_re, c_im, read)
    parts = lax.all_to_all(answer.reshape(ways, -1, LANES), "tp", 0, 0, tiled=True)
    values = parts.astype(F32)
    mean = jnp.sum(values * values, axis=(0, 2), keepdims=True) * (1.0 / (ways * LANES))
    shaped = (values * lax.rsqrt(mean + 1e-06) * out_gain.reshape(ways, 1, LANES)).astype(BF16)
    return jnp.einsum(
        "ktc,kcd->td", shaped, out_proj.reshape(ways, LANES, -1), preferred_element_type=F32
    ).astype(BF16)


def solution(mesh):
    shape = mesh.shape
    chips = shape["sp"] // 2
    near = min(BLOCK, chips)
    devices = mesh.devices.reshape(shape["grp"], chips // near, near, 2, shape["tp"])
    fine_mesh = Mesh(devices, ("grp", "zh", "zl", "core", "tp"))
    rows = ("grp", "zh", "zl", "core", "tp")
    placed = (
        P(rows, None),
        P(("grp", "zh", "zl", "core")),
        P(),
        P(None, "tp"),
        P("tp", None),
        P("tp", None),
        P(None, "tp", None, None),
        P(None, "tp", None, None),
        P(),
        P(),
    )
    return jax.shard_map(
        on_device,
        mesh=fine_mesh,
        in_specs=placed,
        out_specs=P(rows, None),
        check_vma=False,
    )
```
